32 devices in a mesh: kv: 4 (over y, x), tp: 8 (over z, core).
Axes of the slice: x: 2, y: 2, z: 4, core: 2. Of those that a mesh axis runs over, the one named last changes fastest.
Arguments:
- tokens: bfloat16 [128, 4096], P(None, 'tp'), may hold values from -6 to 6
- norm_gain: float32 [4096], P('tp'), may hold values from 0.1 to 1.9
- query_weight: bfloat16 [4096, 2048], P('tp', 'kv'), may hold values from -0.09375 to 0.09375
- key_weight: bfloat16 [4096, 2048], P('tp', 'kv'), may hold values from -0.09375 to 0.09375
- value_weight: bfloat16 [4096, 2048], P('tp', 'kv'), may hold values from -0.09375 to 0.09375
- input_gate_weight: bfloat16 [4096, 16], P('tp'), may hold values from -0.09375 to 0.09375
- forget_gate_weight: bfloat16 [4096, 16], P('tp'), may hold values from -0.09375 to 0.09375
- input_gate_bias: float32 [16], P('kv'), may hold values from -2 to 2
- forget_gate_bias: float32 [16], P('kv'), may hold values from 1 to 6
- memory_state: float32 [128, 16, 128, 128], P('tp', 'kv'), may hold values from -12 to 12
- normalizer_state: float32 [128, 16, 128], P('tp', 'kv'), may hold values from -24 to 24
- stabilizer_state: float32 [128, 16], P('tp', 'kv'), may hold values from -1 to 3
- block_keys: bfloat16 [128, 16, 128, 128], P('tp', 'kv'), may hold values from -6 to 6
- block_values: bfloat16 [128, 16, 128, 128], P('tp', 'kv'), may hold values from -6 to 6
- block_input_pre: float32 [128, 16, 128], P('tp', 'kv'), may hold values from -6 to 6
- block_forget_pre: float32 [128, 16, 128], P('tp', 'kv'), may hold values from -6 to 6
- block_lengths: int32 [128], P('tp'), may hold values from 1 to 128, 6553 in all
- head_norm_gain: float32 [2048], P('kv'), may hold values from 0.1 to 1.9
- output_weight: bfloat16 [2048, 4096], P('kv', 'tp'), may hold values from -0.125 to 0.125
- mixer_norm_gain: float32 [4096], P('tp'), may hold values from 0.1 to 1.9
- gate_weight: bfloat16 [4096, 11264], P('tp', 'kv'), may hold values from -0.09375 to 0.09375
- up_weight: bfloat16 [4096, 11264], P('tp', 'kv'), may hold values from -0.09375 to 0.09375
- down_weight: bfloat16 [11264, 4096], P('kv', 'tp'), may hold values from -0.0546875 to 0.0546875
Outputs:
- layer_output: float32 [128, 4096], P(None, 'tp')
The draws below stay inside these ranges and needn't reach their ends.
Inputs may be any that keep to these rules, and one draw needn't show every extreme that they name: `block_lengths`: some sequence has exactly 128 live positions.
All inputs are finite; a program needn't handle non-finite values. No bound on the sum of `block_lengths` on one device may be relied on, other than what follows from the above.
Results may differ from the reference program's by a relative error of at most 0.0078.
Values may be sent and summed in bfloat16 or wider, within the bound.
No kernel may reach another device: no remote copies, remote signals or barrier semaphores. Data moves between devices by JAX's collectives and lax.ppermute only.
A program may use at most 64 MiB of HBM per device.

```python
import math
import jax
import jax.numpy as jnp
import numpy as np
from jax import lax

D = 4096
H = 16
DH = 128
FF = 11264
BLK = 128
WIDTH = 2048
SEQS = 128


def block_levels(own_key, extent, cuts, least, high):
    loudness = 1.0
    for axis_at, blocks in cuts:
        draws = jax.random.uniform(jax.random.fold_in(jax.random.fold_in(own_key, 6), axis_at), (blocks,), jnp.float32, least / len(cuts), high / len(cuts))
        loudness = loudness * jnp.repeat(jnp.exp(draws), extent[axis_at] // blocks).reshape((-1,) + (1,) * (len(extent) - 1 - axis_at))
    return loudness


def length_profile(number_of, total, reach, lean):
    loads = [(1 << 20) // math.isqrt(grade ** lean) + 1 for grade in range(2, number_of + 1)]
    rest, holding = total - reach - (number_of - 1), [1] * (number_of - 1)
    while rest > 0:
        free = [i for i in range(number_of - 1) if holding[i] < reach]
        whole, remaining = sum([loads[i] for i in free]), rest
        for i in free:
            more = min(reach - holding[i], max(1, remaining * loads[i] // whole), rest)
            holding[i] = holding[i] + more
            rest = rest - more
    return np.array([reach] + holding)


def uneven_parts(own_key, number_of, total, reach, skew):
    if number_of == 2:
        one = jax.random.randint(own_key, (), max(1, total - reach), min(reach, total - 1) + 1)
        return jnp.stack([one, total - one])
    tallies = jnp.asarray(length_profile(number_of, total, reach, skew), jnp.int32)
    pairs = (number_of - 1) // 2
    giver, receiver = tallies[1:1 + 2 * pairs:2], tallies[2:2 + 2 * pairs:2]
    room = jnp.minimum(giver - 1, reach - receiver)
    shifted = jax.random.randint(jax.random.fold_in(own_key, 1), (pairs,), 0, 1 << 20) % (room + 1)
    tallies = tallies.at[1:1 + 2 * pairs:2].set(giver - shifted).at[2:2 + 2 * pairs:2].set(receiver + shifted)
    return tallies[jax.random.permutation(jax.random.fold_in(own_key, 2), number_of)]


def centred(key, shape, scale, most, shards=(), dtype=jnp.bfloat16):
    level = block_levels(key, shape, shards, -0.22, 0.18) if shards else 1.0
    entries = jax.random.normal(key, shape, jnp.float32) * scale * level
    return jnp.minimum(jnp.maximum(entries, -most), most).astype(dtype)


def setup_inputs(seed: int = 0) -> dict:
    streams_of = jax.random.split(jax.random.key(seed), 24)
    return {
        "tokens": centred(streams_of[0], (SEQS, D), 1.0, 6.0, ((1, 8),)),
        "norm_gain": jnp.clip(1.0 + 0.18 * jax.random.normal(streams_of[1], (D,), jnp.float32), 0.1, 1.9),
        "query_weight": centred(streams_of[2], (D, WIDTH), D ** -0.5, 0.09375, ((0, 8), (1, 4))),
        "key_weight": centred(streams_of[3], (D, WIDTH), D ** -0.5, 0.09375, ((0, 8), (1, 4))),
        "value_weight": centred(streams_of[4], (D, WIDTH), D ** -0.5, 0.09375, ((0, 8), (1, 4))),
        "input_gate_weight": centred(streams_of[5], (D, H), D ** -0.5, 0.09375, ((0, 8),)),
        "forget_gate_weight": centred(streams_of[6], (D, H), D ** -0.5, 0.09375, ((0, 8),)),
        "input_gate_bias": jnp.clip(jax.random.uniform(streams_of[7], (H,), jnp.float32, -2.0, 2.0) * block_levels(streams_of[7], (H,), ((0, 4),), -0.4, 0.0), -2.0, 2.0),
        "forget_gate_bias": jnp.clip(1.0 + 5.0 * jax.random.uniform(streams_of[8], (H,), jnp.float32) ** block_levels(streams_of[8], (H,), ((0, 4),), -0.2, 0.2), 1.0, 6.0),
        "memory_state": centred(streams_of[9], (SEQS, H, DH, DH), 2.0, 12.0, ((0, 8), (1, 4)), jnp.float32),
        "normalizer_state": centred(streams_of[10], (SEQS, H, DH), 4.0, 24.0, ((0, 8), (1, 4)), jnp.float32),
        "stabilizer_state": jnp.clip(-1.0 + 4.0 * jax.random.uniform(streams_of[11], (SEQS, H), jnp.float32) ** block_levels(streams_of[11], (SEQS, H), ((0, 8), (1, 4)), -0.2, 0.2), -1.0, 3.0),
        "block_keys": centred(streams_of[12], (SEQS, H, BLK, DH), 1.0, 6.0, ((0, 8), (1, 4))),
        "block_values": centred(streams_of[13], (SEQS, H, BLK, DH), 1.0, 6.0, ((0, 8), (1, 4))),
        "block_input_pre": centred(streams_of[14], (SEQS, H, BLK), 1.0, 6.0, ((0, 8), (1, 4)), jnp.float32),
        "block_forget_pre": centred(streams_of[15], (SEQS, H, BLK), 1.0, 6.0, ((0, 8), (1, 4)), jnp.float32),
        "block_lengths": uneven_parts(streams_of[16], SEQS, SEQS * BLK * 2 // 5, BLK, 2).astype(jnp.int32),
        "head_norm_gain": jnp.clip(1.0 + 0.18 * jax.random.normal(streams_of[17], (WIDTH,), jnp.float32), 0.1, 1.9),
        "output_weight": centred(streams_of[18], (WIDTH, D), WIDTH ** -0.5, 0.125, ((0, 4), (1, 8))),
        "mixer_norm_gain": jnp.clip(1.0 + 0.18 * jax.random.normal(streams_of[19], (D,), jnp.float32), 0.1, 1.9),
        "gate_weight": centred(streams_of[20], (D, FF), D ** -0.5, 0.09375, ((0, 8), (1, 4))),
        "up_weight": centred(streams_of[21], (D, FF), D ** -0.5, 0.09375, ((0, 8), (1, 4))),
        "down_weight": centred(streams_of[22], (FF, D), FF ** -0.5, 0.0546875, ((0, 4), (1, 8))),
    }


epsilon = 1e-06

def memory_cell(queries, new_keys, new_values, log_input, log_forget, memory, normalizer, stabilizer, cached_keys, cached_values, input_pre, forget_pre, lengths, input_bias, forget_bias):
    positions = jnp.arange(cached_keys.shape[2])
    is_live = (positions[None, :] < lengths[:, None])[:, None, :]
    cached_input = input_pre + input_bias[None, :, None]
    cached_forget = jnp.where(is_live, jax.nn.log_sigmoid(forget_pre + forget_bias[None, :, None]), 0.0)
    after_mask = (positions[:, None] > positions[None, :]).astype(jnp.float32)
    later_forget = jnp.einsum('bhu,us->bhs', cached_forget, after_mask, precision=lax.Precision.HIGHEST) + log_forget[..., None]
    total_forget = lax.optimization_barrier(jnp.sum(cached_forget, axis=-1)) + log_forget
    exponent = jnp.where(is_live, later_forget + cached_input, -jnp.inf)
    carried = total_forget + stabilizer
    stab_max = jnp.maximum(jnp.maximum(lax.optimization_barrier(jnp.max(exponent, axis=-1)), carried), log_input)
    query_wide = queries.astype(jnp.float32)
    scores = jnp.einsum('bhd,bhsd->bhs', query_wide, cached_keys.astype(jnp.float32))
    block_weight = jnp.exp(exponent - stab_max[..., None]) * scores
    block_probs = block_weight.astype(jnp.bfloat16)
    block_sum = jnp.einsum('bhs,bhsd->bhd', block_probs.astype(jnp.float32), cached_values.astype(jnp.float32))
    new_weight = jnp.exp(log_input - stab_max) * lax.optimization_barrier(jnp.sum(query_wide * new_keys.astype(jnp.float32), axis=-1))
    state_weight = jnp.exp(carried - stab_max)
    state_sum = jnp.einsum('bhkv,bhk->bhv', memory, query_wide, precision=lax.Precision.HIGHEST)
    state_norm = lax.optimization_barrier(jnp.sum(normalizer * query_wide, axis=-1))
    numerator = block_sum + new_weight[..., None] * new_values.astype(jnp.float32) + state_weight[..., None] * state_sum
    denominator = lax.optimization_barrier(jnp.sum(block_weight, axis=-1)) + new_weight + state_weight * state_norm
    return numerator / jnp.maximum(jnp.abs(denominator), 1.0)[..., None]

def head_scale(cell_out, gain):
    return (cell_out * gain.reshape(cell_out.shape[1], cell_out.shape[2])).astype(jnp.bfloat16)

def reference(tokens, norm_gain, query_weight, key_weight, value_weight, input_gate_weight, forget_gate_weight, input_gate_bias, forget_gate_bias, memory_state, normalizer_state, stabilizer_state, block_keys, block_values, block_input_pre, block_forget_pre, block_lengths, head_norm_gain, output_weight, mixer_norm_gain, gate_weight, up_weight, down_weight):
    seq_rows = tokens.shape[0]
    tok_wide = tokens.astype(jnp.float32)
    first_scale = lax.rsqrt(lax.optimization_barrier(jnp.mean(tok_wide * tok_wide, axis=1)) + epsilon)[:, None]
    scaled_in = (tok_wide * norm_gain).astype(jnp.bfloat16)

    def project(weight):
        return jnp.dot(scaled_in, weight, preferred_element_type=jnp.float32) * first_scale
    queries = (project(query_weight) * DH ** (-0.5)).astype(jnp.bfloat16).reshape(seq_rows, H, DH)
    new_keys = project(key_weight).astype(jnp.bfloat16).reshape(seq_rows, H, DH)
    new_values = project(value_weight).astype(jnp.bfloat16).reshape(seq_rows, H, DH)
    log_input = project(input_gate_weight) + input_gate_bias
    log_forget = jax.nn.log_sigmoid(project(forget_gate_weight) + forget_gate_bias)
    cell_out = memory_cell(queries, new_keys, new_values, log_input, log_forget, memory_state, normalizer_state, stabilizer_state, block_keys, block_values, block_input_pre, block_forget_pre, block_lengths, input_gate_bias, forget_gate_bias)
    head_out = head_scale(cell_out, head_norm_gain).reshape(seq_rows, H * DH)
    attended = jnp.dot(head_out, output_weight, preferred_element_type=jnp.float32)
    res_wide = tok_wide + attended
    second_scale = lax.rsqrt(lax.optimization_barrier(jnp.mean(res_wide * res_wide, axis=1)) + epsilon)[:, None]
    mid_scaled = (res_wide * mixer_norm_gain).astype(jnp.bfloat16)
    gate_pre = jnp.dot(mid_scaled, gate_weight, preferred_element_type=jnp.float32) * second_scale
    up_pre = jnp.dot(mid_scaled, up_weight, preferred_element_type=jnp.float32) * second_scale
    hidden = (jax.nn.silu(gate_pre) * up_pre).astype(jnp.bfloat16)
    mixed = jnp.dot(hidden, down_weight, preferred_element_type=jnp.float32)
    return res_wide + mixed
```

```python
import functools

import jax
import jax.numpy as jnp
from jax import lax
from jax.experimental import pallas as pl
from jax.experimental.pallas import tpu as pltpu
from jax.sharding import PartitionSpec as P


f32 = jnp.float32
bf16 = jnp.bfloat16
epsilon = 1e-06
LANES = 128
VMEM = pl.BlockSpec(memory_space=pltpu.VMEM)


def size_of(x):
    n = x.dtype.itemsize
    for extent in x.shape:
        n *= extent
    return n


def call(kernel, ins, outs, scratch=(), flops=1):
    total = sum(size_of(x) for x in ins) + sum(size_of(x) for x in outs)
    total += sum(size_of(x) for x in scratch)
    return pl.pallas_call(
        kernel,
        out_shape=list(outs),
        in_specs=[VMEM] * len(ins),
        out_specs=[VMEM] * len(outs),
        scratch_shapes=[pltpu.VMEM(s.shape, s.dtype) for s in scratch],
        compiler_params=pltpu.CompilerParams(vmem_limit_bytes=min(total + total // 4 + (6 << 20), 60 << 20)),
        cost_estimate=pl.CostEstimate(flops=flops, bytes_accessed=total, transcendentals=0),
    )(*ins)


def sds(shape, dtype):
    return jax.ShapeDtypeStruct(shape, dtype)


def digits_of(n, first=2):
    out, shift = [], 0
    left = n
    while left > 1:
        radix = min(2 if shift == 0 and first == 1 else 4, left)
        assert left % radix == 0 and radix in (2, 4)
        out.append((shift, radix))
        shift += radix.bit_length() - 1
        left //= radix
    return out


def swap(x, axis, n, mask):
    return lax.ppermute(x, axis, [(i, i ^ mask) for i in range(n)])


def digit_index(axis, shift, radix):
    return lax.rem(lax.div(lax.axis_index(axis), jnp.int32(1 << shift)), jnp.int32(radix))


def rows_at(index, rows):
    return pl.ds(pl.multiple_of(index * rows, rows), rows)


def join_tail(tail):
    return tail + pltpu.roll(tail, LANES // 2, 1)


def split_tail(both):
    lane = lax.broadcasted_iota(jnp.int32, both.shape, 1)
    high = both.astype(bf16).astype(f32)
    return jnp.where(lane < LANES // 2, high, both - high).astype(bf16)


def keep_tail(both):
    lane = lax.broadcasted_iota(jnp.int32, both.shape, 1)
    return jnp.where(lane < LANES // 2, both, 0.0)


def project_kernel(rows, tok, gain, wq, wk, wv, wi, wf, keep, send, perm):
    total = tok.shape[0]
    half = total // 2
    width = wq.shape[1]
    core = digit_index("tp", 0, 2)
    for z in range(half // rows):
        perm[z * rows : (z + 1) * rows, :] = tok[rows_at(2 * z + core, rows), :]
        perm[half + z * rows : half + (z + 1) * rows, :] = tok[rows_at(2 * z + 1 - core, rows), :]
    wide = perm[...].astype(f32)
    scaled = (wide * gain[...]).astype(bf16)
    squares = jnp.sum(wide * wide, axis=1, keepdims=True)

    def product(w):
        return jnp.dot(scaled, w[...], preferred_element_type=f32)

    for i, w in enumerate((wq, wk, wv)):
        p = product(w)
        keep[:, i * width : (i + 1) * width] = p[:half]
        send[:, i * width : (i + 1) * width] = p[half:].astype(bf16)
    heads = wi.shape[1]
    blank = jnp.zeros((total, LANES // 2 - 2 * heads - 1), f32)
    tail = jnp.concatenate([product(wi), product(wf), squares, blank] * 2, axis=1)
    keep[:, 3 * width :] = keep_tail(tail[:half])
    send[:, 3 * width :] = split_tail(tail[half:])


def split_kernel(rows, shift, radix, n_recv, *refs):
    acc, recvs = refs[0], refs[1 : 1 + n_recv]
    mine, sends = refs[1 + n_recv], refs[2 + n_recv :]
    body = acc.shape[1] - LANES
    digit = digit_index("tp", shift, radix)
    for block in range(acc.shape[0] // (radix * rows)):
        to = slice(block * rows, (block + 1) * rows)
        for k in range(radix):
            at = rows_at(block * radix + (digit ^ k), rows)
            value = acc[at, :]
            for r in recvs:
                value = value + r[at, :].astype(f32)
            if k == 0:
                mine[to, :] = value
            else:
                sends[k - 1][to, :body] = value[:, :body].astype(bf16)
                sends[k - 1][to, body:] = split_tail(join_tail(value[:, body:]))


def gating_kernel(ipre, fpre, lens, stab, bias_i, bias_f, e0, carried, top):
    seqs, heads, block = ipre.shape
    row = lax.broadcasted_iota(jnp.int32, (seqs, seqs), 0)
    lane = lax.broadcasted_iota(jnp.int32, (seqs, seqs), 1)
    own = jnp.where(row == lane, lens[...].astype(f32), 0.0)
    length = jnp.sum(own, axis=1, keepdims=True)
    position = lax.broadcasted_iota(jnp.int32, (seqs, block), 1).astype(f32)
    live = position < length
    before = lax.broadcasted_iota(jnp.int32, (block, block), 0)
    after = lax.broadcasted_iota(jnp.int32, (block, block), 1)
    mask = (before > after).astype(f32)
    for h in range(heads):
        to = slice(h * seqs, (h + 1) * seqs)
        pre = fpre[:, h, :] + bias_f[:, h : h + 1]
        log_sig = jnp.minimum(pre, 0.0) - jnp.log1p(jnp.exp(-jnp.abs(pre)))
        forget = jnp.where(live, log_sig, 0.0)
        later = jnp.dot(forget, mask, precision=lax.Precision.HIGHEST, preferred_element_type=f32)
        exponent = jnp.where(live, later + (ipre[:, h, :] + bias_i[:, h : h + 1]), -jnp.inf)
        state = jnp.sum(forget, axis=1, keepdims=True) + stab[:, h : h + 1]
        e0[to, :] = exponent
        carried[to, :] = jnp.broadcast_to(state, exponent.shape)
        largest = jnp.maximum(jnp.max(exponent, axis=1, keepdims=True), state)
        top[to, :] = jnp.broadcast_to(largest, exponent.shape)


def cell_kernel(model, n_recv, *refs):
    acc, recvs = refs[0], refs[1 : 1 + n_recv]
    e0, carried, top, keys, values, memory, normalizer, bias_i, bias_f, gain, out = refs[1 + n_recv :]
    seqs, heads, size = normalizer.shape
    width = heads * size
    all_heads = model[1]

    def columns(start, stop):
        value = acc[:, start:stop]
        for r in recvs:
            value = value + r[:, start:stop].astype(f32)
        return value

    tail = join_tail(columns(3 * width, 3 * width + LANES))
    lane = lax.broadcasted_iota(jnp.int32, tail.shape, 1)

    def pick(at):
        return jnp.sum(jnp.where(lane == at, tail, 0.0), axis=1, keepdims=True)

    scale = lax.rsqrt(tail[:, 2 * all_heads : 2 * all_heads + 1] / model[0] + epsilon)
    first = lax.axis_index("kv") * heads
    row = lax.broadcasted_iota(jnp.int32, (seqs, size), 0)
    for h in range(heads):
        at = slice(h * size, (h + 1) * size)
        to = slice(h * seqs, (h + 1) * seqs)
        in_lane = first + h
        log_input = pick(in_lane) * scale + bias_i[:, h : h + 1]
        pre = pick(in_lane + all_heads) * scale + bias_f[:, h : h + 1]
        log_forget = jnp.minimum(pre, 0.0) - jnp.log1p(jnp.exp(-jnp.abs(pre)))
        stab_max = jnp.maximum(top[to, :] + log_forget, log_input)
        query = (columns(at.start, at.stop) * scale * size ** (-0.5)).astype(bf16)
        new_key = (columns(width + at.start, width + at.stop) * scale).astype(bf16).astype(f32)
        new_value = (columns(2 * width + at.start, 2 * width + at.stop) * scale).astype(bf16).astype(f32)
        wide = query.astype(f32)
        scores = jnp.zeros((seqs, size), f32)
        state_sum = jnp.zeros((seqs, size), f32)
        for b in range(seqs):
            s = lax.dot_general(query, keys[b, h], (((1,), (1,)), ((), ())), preferred_element_type=f32)
            scores = jnp.where(row == b, s, scores)
            cells = memory[b, h]
            high = cells.astype(bf16)
            low = (cells - high.astype(f32)).astype(bf16)
            m = jnp.dot(query, high, preferred_element_type=f32) + jnp.dot(query, low, preferred_element_type=f32)
            state_sum = jnp.where(row == b, m, state_sum)
        weight = jnp.exp(e0[to, :] + log_forget - stab_max) * scores
        probs = weight.astype(bf16)
        block_sum = jnp.zeros((seqs, size), f32)
        for b in range(seqs):
            p = jnp.dot(probs, values[b, h], preferred_element_type=f32)
            block_sum = jnp.where(row == b, p, block_sum)
        new_weight = jnp.exp(log_input - stab_max) * jnp.sum(wide * new_key, axis=1, keepdims=True)
        state_weight = jnp.exp(carried[to, :] + log_forget - stab_max)
        state_norm = jnp.sum(normalizer[:, h, :] * wide, axis=1, keepdims=True)
        numerator = block_sum + new_weight * new_value + state_weight * state_sum
        denominator = jnp.sum(weight, axis=1, keepdims=True) + new_weight + state_weight * state_norm
        cell = numerator / jnp.maximum(jnp.abs(denominator), 1.0)
        out[:, at] = (cell * gain[:, at]).astype(bf16)


def place_rows(masks, rows, near, far, whole):
    me = lax.axis_index("tp")
    for i, mask in enumerate(masks):
        part, j = (near, i) if i < len(masks) // 2 else (far, i - len(masks) // 2)
        whole[rows_at(me ^ mask, rows), :] = part[j * rows : (j + 1) * rows, :]


def apply_kernel(masks, rows, near, far, w, out, whole):
    place_rows(masks, rows, near, far, whole)
    out[...] = jnp.dot(whole[...], w[...], preferred_element_type=f32).astype(bf16)


def tree(values):
    while len(values) > 1:
        values = [a + b for a, b in zip(values[::2], values[1::2])]
    return values[0]


def mixer_kernel(rows, n_terms, *refs):
    terms = refs[:n_terms]
    tok, gain, wg, wu, res, keep, send, perm = refs[n_terms:]
    total = tok.shape[0]
    half = total // 2
    width = wg.shape[1]
    padded = (keep.shape[1] - LANES) // 2
    core = digit_index("tp", 0, 2)
    value = tok[...].astype(f32) + tree([t[...].astype(f32) for t in terms])
    res[...] = value
    for z in range(half // rows):
        perm[z * rows : (z + 1) * rows, :] = res[rows_at(2 * z + core, rows), :]
        perm[half + z * rows : half + (z + 1) * rows, :] = res[rows_at(2 * z + 1 - core, rows), :]
    wide = perm[...]
    squares = jnp.broadcast_to(jnp.sum(wide * wide, axis=1, keepdims=True), (total, LANES))
    scaled = (wide * gain[...]).astype(bf16)
    for i, w in enumerate((wg, wu)):
        for start in range(0, width, 512):
            stop = min(start + 512, width)
            p = jnp.dot(scaled, w[:, start:stop], preferred_element_type=f32)
            keep[:, i * padded + start : i * padded + stop] = p[:half]
            send[:, i * padded + start : i * padded + stop] = p[half:].astype(bf16)
    keep[:, 2 * padded :] = keep_tail(squares[:half])
    send[:, 2 * padded :] = split_tail(squares[half:])


def activate_kernel(model, n_recv, *refs):
    acc, recvs, out = refs[0], refs[1 : 1 + n_recv], refs[1 + n_recv]
    width = out.shape[1]
    padded = (acc.shape[1] - LANES) // 2

    def columns(start, stop):
        value = acc[:, start:stop]
        for r in recvs:
            value = value + r[:, start:stop].astype(f32)
        return value

    tail = join_tail(columns(2 * padded, 2 * padded + LANES))
    scale = lax.rsqrt(tail[:, :1] / model + epsilon)
    gate = columns(0, width) * scale
    up = columns(padded, padded + width) * scale
    out[...] = (gate / (1.0 + jnp.exp(-gate)) * up).astype(bf16)


def scatter_rounds(keep, send, rows, tp):
    width = keep.shape[1]
    acc, recvs = keep, [swap(send, "tp", tp, 1)]
    for shift, radix in digits_of(tp, 1)[1:]:
        n_out = acc.shape[0] // radix
        outs = [sds((n_out, width), f32)] + [sds((n_out, width), bf16)] * (radix - 1)
        got = call(
            functools.partial(split_kernel, rows, shift, radix, len(recvs)),
            [acc, *recvs],
            outs,
        )
        acc = got[0]
        recvs = [swap(s, "tp", tp, k << shift) for k, s in enumerate(got[1:], 1)]
    return acc, recvs


def gather_rounds(x, tp):
    masks = [0]
    for shift, radix in digits_of(tp, 1)[1:]:
        x = jnp.concatenate([x] + [swap(x, "tp", tp, k << shift) for k in range(1, radix)], axis=0)
        masks = [m | (k << shift) for k in range(radix) for m in masks]
    return x, swap(x, "tp", tp, 1), masks + [m | 1 for m in masks]


def sum_terms(part, kv):
    digits = digits_of(kv)
    terms = [part]
    for i, (shift, radix) in enumerate(digits):
        if i:
            part = tree([t.astype(f32) for t in terms]).astype(bf16)
        terms = [part] + [swap(part, "kv", kv, k << shift) for k in range(1, radix)]
    return terms


def solution(mesh):
    tp, kv = mesh.shape["tp"], mesh.shape["kv"]

    def body(
        tokens,
        norm_gain,
        query_weight,
        key_weight,
        value_weight,
        input_gate_weight,
        forget_gate_weight,
        input_gate_bias,
        forget_gate_bias,
        memory_state,
        normalizer_state,
        stabilizer_state,
        block_keys,
        block_values,
        block_input_pre,
        block_forget_pre,
        block_lengths,
        head_norm_gain,
        output_weight,
        mixer_norm_gain,
        gate_weight,
        up_weight,
        down_weight,
    ):
        total, depth = tokens.shape
        seqs, heads, block, size = block_keys.shape
        width = heads * size
        model = depth * tp
        all_heads = input_gate_weight.shape[1]
        half = total // 2
        bias_i, bias_f = input_gate_bias[None, :], forget_gate_bias[None, :]

        packed = 3 * width + LANES
        keep, send = call(
            functools.partial(project_kernel, seqs),
            [
                tokens,
                norm_gain[None, :],
                query_weight,
                key_weight,
                value_weight,
                input_gate_weight,
                forget_gate_weight,
            ],
            [sds((half, packed), f32), sds((half, packed), bf16)],
            [sds((total, depth), bf16)],
        )
        acc, recvs = scatter_rounds(keep, send, seqs, tp)
        e0, carried, top = call(
            gating_kernel,
            [
                block_input_pre,
                block_forget_pre,
                block_lengths[None, :],
                stabilizer_state,
                bias_i,
                bias_f,
            ],
            [sds((heads * seqs, block), f32)] * 3,
        )
        (head_out,) = call(
            functools.partial(cell_kernel, (float(model), all_heads), len(recvs)),
            [
                acc,
                *recvs,
                e0,
                carried,
                top,
                block_keys,
                block_values,
                memory_state,
                normalizer_state,
                bias_i,
                bias_f,
                head_norm_gain[None, :],
            ],
            [sds((seqs, width), bf16)],
        )
        near, far, masks = gather_rounds(head_out, tp)
        (part,) = call(
            functools.partial(apply_kernel, masks, seqs),
            [near, far, output_weight],
            [sds((total, depth), bf16)],
            [sds((total, width), bf16)],
        )
        terms = sum_terms(part, kv)

        hidden_dev = gate_weight.shape[1]
        padded = pl.cdiv(hidden_dev, LANES) * LANES
        packed = 2 * padded + LANES
        res, keep, send = call(
            functools.partial(mixer_kernel, seqs, len(terms)),
            [*terms, tokens, mixer_norm_gain[None, :], gate_weight, up_weight],
            [sds((total, depth), f32), sds((half, packed), f32), sds((half, packed), bf16)],
            [sds((total, depth), f32)],
        )
        acc, recvs = scatter_rounds(keep, send, seqs, tp)
        (hidden,) = call(
            functools.partial(activate_kernel, float(model), len(recvs)),
            [acc, *recvs],
            [sds((seqs, hidden_dev), bf16)],
        )
        near, far, masks = gather_rounds(hidden, tp)
        (part,) = call(
            functools.partial(apply_kernel, masks, seqs),
            [near, far, down_weight],
            [sds((total, depth), bf16)],
            [sds((total, hidden_dev), bf16)],
        )
        terms = sum_terms(part, kv)
        return res + tree([t.astype(f32) for t in terms])

    placed = (
        P(None, "tp"),
        P("tp"),
        P("tp", "kv"),
        P("tp", "kv"),
        P("tp", "kv"),
        P("tp", None),
        P("tp", None),
        P("kv"),
        P("kv"),
        P("tp", "kv", None, None),
        P("tp", "kv", None),
        P("tp", "kv"),
        P("tp", "kv", None, None),
        P("tp", "kv", None, None),
        P("tp", "kv", None),
        P("tp", "kv", None),
        P("tp"),
        P("kv"),
        P("kv", "tp"),
        P("tp"),
        P("tp", "kv"),
        P("tp", "kv"),
        P("kv", "tp"),
    )
    return jax.shard_map(body, mesh=mesh, in_specs=placed, out_specs=P(None, "tp"), check_vma=False)
```

```python
import functools

import jax
import jax.numpy as jnp
from jax import lax
from jax.experimental import pallas as pl
from jax.experimental.pallas import tpu as pltpu
from jax.sharding import PartitionSpec as P


f32 = jnp.float32
bf16 = jnp.bfloat16
epsilon = 1e-06
LANES = 128
VMEM = pl.BlockSpec(memory_space=pltpu.VMEM)
HBM = pl.BlockSpec(memory_space=pltpu.HBM)


def size_of(x):
    n = x.dtype.itemsize
    for extent in x.shape:
        n *= extent
    return n


def call(kernel, ins, outs, scratch=(), flops=1, fetched=(), copies=0):
    total = sum(size_of(x) for x in ins) + sum(size_of(x) for x in outs)
    total += sum(size_of(x) for x in scratch)
    shapes = [pltpu.VMEM(s.shape, s.dtype) for s in scratch]
    if copies:
        shapes.append(pltpu.SemaphoreType.DMA((copies,)))
    return pl.pallas_call(
        kernel,
        out_shape=list(outs),
        in_specs=[HBM if i in fetched else VMEM for i in range(len(ins))],
        out_specs=[VMEM] * len(outs),
        scratch_shapes=shapes,
        compiler_params=pltpu.CompilerParams(vmem_limit_bytes=min(total + total // 4 + (6 << 20), 60 << 20)),
        cost_estimate=pl.CostEstimate(flops=flops, bytes_accessed=total, transcendentals=0),
    )(*[pinned(x) if i in fetched else x for i, x in enumerate(ins)])


def pinned(x):
    return pltpu.with_memory_space_constraint(x, pltpu.HBM) if x.size > 1 else x


def start_copies(pairs, sems):
    copies = [pltpu.make_async_copy(a, b, sems.at[i]) for i, (a, b) in enumerate(pairs)]
    for c in copies:
        c.start()
    return copies


def sds(shape, dtype):
    return jax.ShapeDtypeStruct(shape, dtype)


def digits_of(n, first=2):
    out, shift = [], 0
    left = n
    while left > 1:
        radix = min(2 if shift == 0 and first == 1 else 4, left)
        assert left % radix == 0 and radix in (2, 4)
        out.append((shift, radix))
        shift += radix.bit_length() - 1
        left //= radix
    return out


def swap(x, axis, n, mask):
    return lax.ppermute(x, axis, [(i, i ^ mask) for i in range(n)])


def digit_index(axis, shift, radix):
    return lax.rem(lax.div(lax.axis_index(axis), jnp.int32(1 << shift)), jnp.int32(radix))


def rows_at(index, rows):
    return pl.ds(pl.multiple_of(index * rows, rows), rows)


def join_tail(tail):
    return tail + pltpu.roll(tail, LANES // 2, 1)


def split_tail(both):
    lane = lax.broadcasted_iota(jnp.int32, both.shape, 1)
    high = both.astype(bf16).astype(f32)
    return jnp.where(lane < LANES // 2, high, both - high).astype(bf16)


def keep_tail(both):
    lane = lax.broadcasted_iota(jnp.int32, both.shape, 1)
    return jnp.where(lane < LANES // 2, both, 0.0)


def project_kernel(rows, *refs):
    hbm, (keep, send), local = refs[:7], refs[7:9], refs[9:16]
    perm, sems = refs[16:]
    copies = start_copies(list(zip(hbm, local)), sems)
    tok, gain, wq, wk, wv, wi, wf = local
    total = tok.shape[0]
    half = total // 2
    width = wq.shape[1]
    core = digit_index("tp", 0, 2)
    copies[0].wait()
    copies[1].wait()
    for z in range(half // rows):
        perm[z * rows : (z + 1) * rows, :] = tok[rows_at(2 * z + core, rows), :]
        perm[half + z * rows : half + (z + 1) * rows, :] = tok[rows_at(2 * z + 1 - core, rows), :]
    wide = perm[...].astype(f32)
    scaled = (wide * gain[...]).astype(bf16)
    squares = jnp.sum(wide * wide, axis=1, keepdims=True)
    for i, w in enumerate((wq, wk, wv)):
        copies[2 + i].wait()
        p = jnp.dot(scaled, w[...], preferred_element_type=f32)
        keep[:, i * width : (i + 1) * width] = p[:half]
        send[:, i * width : (i + 1) * width] = p[half:].astype(bf16)
    copies[5].wait()
    copies[6].wait()
    gates = [
        lax.dot_general(scaled, w[...], (((1,), (1,)), ((), ())), preferred_element_type=f32)
        for w in (wi, wf)
    ]
    blank = jnp.zeros((total, LANES // 2 - 2 * wi.shape[0] - 1), f32)
    tail = jnp.concatenate([*gates, squares, blank] * 2, axis=1)
    keep[:, 3 * width :] = keep_tail(tail[:half])
    send[:, 3 * width :] = split_tail(tail[half:])


def split_kernel(rows, shift, radix, n_recv, tail, *refs):
    acc, recvs = refs[0], refs[1 : 1 + n_recv]
    mine, sends = refs[1 + n_recv], refs[2 + n_recv :]
    body = acc.shape[1] - LANES * tail
    digit = digit_index("tp", shift, radix)
    for block in range(acc.shape[0] // (radix * rows)):
        to = slice(block * rows, (block + 1) * rows)
        for k in range(radix):
            at = rows_at(block * radix + (digit ^ k), rows)
            value = acc[at, :]
            for r in recvs:
                value = value + r[at, :].astype(f32)
            if k == 0:
                mine[to, :] = value
            else:
                sends[k - 1][to, :body] = value[:, :body].astype(bf16)
                if tail:
                    sends[k - 1][to, body:] = split_tail(join_tail(value[:, body:]))


def row_to_column(values, seqs):
    row = lax.broadcasted_iota(jnp.int32, (seqs, seqs), 0)
    lane = lax.broadcasted_iota(jnp.int32, (seqs, seqs), 1)
    return jnp.sum(jnp.where(row == lane, values, 0.0), axis=1, keepdims=True)


PIECES = 4


def gating_kernel(*refs):
    small, (keys_in, values_in, memory_in) = refs[:8], refs[8:11]
    e0, carried, top, keys, values, memory, normalizer, gain, biases = refs[11:20]
    local, (wide, sems) = refs[20:26], refs[26:]
    ipre, fpre, lens, stab, bias_i, bias_f = local
    seqs, heads, block = ipre.shape
    size = wide.shape[2]
    per = seqs // PIECES
    pairs = list(zip(small, (*local, normalizer, gain)))
    for i in range(PIECES):
        pairs.append((memory_in.at[i * per : (i + 1) * per], wide.at[i * per : (i + 1) * per]))
    pairs += [(keys_in, keys), (values_in, values)]
    copies = start_copies(pairs, sems)
    for c in copies[:6]:
        c.wait()
    biases[0:1, :heads] = bias_i[...]
    biases[1:2, :heads] = bias_f[...]
    length = row_to_column(lens[...].astype(f32), seqs)
    position = lax.broadcasted_iota(jnp.int32, (seqs, block), 1).astype(f32)
    live = position < length
    before = lax.broadcasted_iota(jnp.int32, (block, block), 0)
    after = lax.broadcasted_iota(jnp.int32, (block, block), 1)
    mask = (before > after).astype(f32)
    for h in range(heads):
        to = slice(h * seqs, (h + 1) * seqs)
        pre = fpre[:, h, :] + bias_f[:, h : h + 1]
        log_sig = jnp.minimum(pre, 0.0) - jnp.log1p(jnp.exp(-jnp.abs(pre)))
        forget = jnp.where(live, log_sig, 0.0)
        later = jnp.dot(forget, mask, precision=lax.Precision.HIGHEST, preferred_element_type=f32)
        exponent = jnp.where(live, later + (ipre[:, h, :] + bias_i[:, h : h + 1]), -jnp.inf)
        state = jnp.sum(forget, axis=1, keepdims=True) + row_to_column(stab[h : h + 1, :], seqs)
        e0[to, :] = exponent
        carried[to, :] = jnp.broadcast_to(state, exponent.shape)
        largest = jnp.maximum(jnp.max(exponent, axis=1, keepdims=True), state)
        top[to, :] = jnp.broadcast_to(largest, exponent.shape)
    for i in range(PIECES):
        copies[8 + i].wait()
        for b in range(i * per, (i + 1) * per):
            for h in range(heads):
                cells = wide[b, h]
                high = cells.astype(bf16)
                memory[b, h, :size, :] = high
                memory[b, h, size:, :] = (cells - high.astype(f32)).astype(bf16)
    for c in (*copies[6:8], *copies[8 + PIECES :]):
        c.wait()


def cell_kernel(model, n_recv, *refs):
    acc, recvs = refs[0], refs[1 : 1 + n_recv]
    e0, carried, top, keys, values, memory, normalizer, gain, biases, out = refs[1 + n_recv :]
    seqs, heads, size = normalizer.shape
    width = heads * size
    all_heads = model[1]

    def columns(start, stop):
        value = acc[:, start:stop]
        for r in recvs:
            value = value + r[:, start:stop].astype(f32)
        return value

    tail = join_tail(columns(3 * width, 3 * width + LANES))
    lane = lax.broadcasted_iota(jnp.int32, tail.shape, 1)

    def pick(at):
        return jnp.sum(jnp.where(lane == at, tail, 0.0), axis=1, keepdims=True)

    scale = lax.rsqrt(tail[:, 2 * all_heads : 2 * all_heads + 1] / model[0] + epsilon)
    first = lax.axis_index("kv") * heads
    row = lax.broadcasted_iota(jnp.int32, (seqs, size), 0)
    for h in range(heads):
        at = slice(h * size, (h + 1) * size)
        to = slice(h * seqs, (h + 1) * seqs)
        in_lane = first + h
        log_input = pick(in_lane) * scale + biases[0:1, h : h + 1]
        pre = pick(in_lane + all_heads) * scale + biases[1:2, h : h + 1]
        log_forget = jnp.minimum(pre, 0.0) - jnp.log1p(jnp.exp(-jnp.abs(pre)))
        stab_max = jnp.maximum(top[to, :] + log_forget, log_input)
        query = (columns(at.start, at.stop) * scale * size ** (-0.5)).astype(bf16)
        new_key = (columns(width + at.start, width + at.stop) * scale).astype(bf16).astype(f32)
        new_value = (columns(2 * width + at.start, 2 * width + at.stop) * scale).astype(bf16).astype(f32)
        wide = query.astype(f32)
        twice = jnp.concatenate([query, query], axis=1)
        scores = jnp.zeros((seqs, size), f32)
        state_sum = jnp.zeros((seqs, size), f32)
        for b in range(seqs):
            s = lax.dot_general(query, keys[b, h], (((1,), (1,)), ((), ())), preferred_element_type=f32)
            scores = jnp.where(row == b, s, scores)
            m = jnp.dot(twice, memory[b, h], preferred_element_type=f32)
            state_sum = jnp.where(row == b, m, state_sum)
        weight = jnp.exp(e0[to, :] + log_forget - stab_max) * scores
        probs = weight.astype(bf16)
        block_sum = jnp.zeros((seqs, size), f32)
        for b in range(seqs):
            p = jnp.dot(probs, values[b, h], preferred_element_type=f32)
            block_sum = jnp.where(row == b, p, block_sum)
        new_weight = jnp.exp(log_input - stab_max) * jnp.sum(wide * new_key, axis=1, keepdims=True)
        state_weight = jnp.exp(carried[to, :] + log_forget - stab_max)
        state_norm = jnp.sum(normalizer[:, h, :] * wide, axis=1, keepdims=True)
        numerator = block_sum + new_weight * new_value + state_weight * state_sum
        denominator = jnp.sum(weight, axis=1, keepdims=True) + new_weight + state_weight * state_norm
        cell = numerator / jnp.maximum(jnp.abs(denominator), 1.0)
        out[:, at] = (cell * gain[:, at]).astype(bf16)


def place_rows(masks, rows, near, far, whole):
    me = lax.axis_index("tp")
    for part, core in ((near, 0), (far, 1)):
        for i, mask in enumerate(masks):
            whole[rows_at(me ^ (mask | core), rows), :] = part[i * rows : (i + 1) * rows, :]


def apply_kernel(masks, rows, near, far, w, out, whole):
    place_rows(masks, rows, near, far, whole)
    out[...] = jnp.dot(whole[...], w[...], preferred_element_type=f32).astype(bf16)


def down_kernel(masks, rows, at, more, *refs):
    near, far, w = refs[:3]
    out, whole = refs[-2:]
    place_rows(masks, rows, near, far, whole)
    width = near.shape[1]
    value = jnp.dot(whole[...], w[at : at + width, :], preferred_element_type=f32)
    if more:
        value = value + refs[3][...]
    out[...] = value.astype(out.dtype)


def tree(values):
    while len(values) > 1:
        values = [a + b for a, b in zip(values[::2], values[1::2])]
    return values[0]


def write_products(scaled, weights, at, width, keep, send):
    half = keep.shape[0]
    padded = pl.cdiv(width, LANES) * LANES
    for i, w in enumerate(weights):
        for start in range(0, width, 512):
            stop = min(start + 512, width)
            p = jnp.dot(scaled, w[:, at + start : at + stop], preferred_element_type=f32)
            keep[:, i * padded + start : i * padded + stop] = p[:half]
            send[:, i * padded + start : i * padded + stop] = p[half:].astype(bf16)


def mixer_kernel(rows, width, n_terms, *refs):
    terms = refs[:n_terms]
    tok, gain, wg, wu, res, scaled, keep, send, perm = refs[n_terms:]
    total = tok.shape[0]
    half = total // 2
    core = digit_index("tp", 0, 2)
    res[...] = tok[...].astype(f32) + tree([t[...].astype(f32) for t in terms])
    for z in range(half // rows):
        perm[z * rows : (z + 1) * rows, :] = res[rows_at(2 * z + core, rows), :]
        perm[half + z * rows : half + (z + 1) * rows, :] = res[rows_at(2 * z + 1 - core, rows), :]
    wide = perm[...]
    squares = jnp.broadcast_to(jnp.sum(wide * wide, axis=1, keepdims=True), (total, LANES))
    keep[:, keep.shape[1] - LANES :] = keep_tail(squares[:half])
    send[:, keep.shape[1] - LANES :] = split_tail(squares[half:])
    scaled[...] = (wide * gain[...]).astype(bf16)
    write_products(scaled[...], (wg, wu), 0, width, keep, send)


def rest_kernel(at, width, scaled, wg, wu, keep, send):
    write_products(scaled[...], (wg, wu), at, width, keep, send)


def activate_kernel(model, n_recv, first, *refs):
    acc, recvs = refs[0], refs[1 : 1 + n_recv]
    if first:
        out, scales = refs[-2:]
    else:
        scales, out = refs[-2:]
    width = out.shape[1]
    padded = pl.cdiv(width, LANES) * LANES

    def columns(start, stop):
        value = acc[:, start:stop]
        for r in recvs:
            value = value + r[:, start:stop].astype(f32)
        return value

    if first:
        tail = join_tail(columns(2 * padded, 2 * padded + LANES))
        scales[...] = lax.rsqrt(tail / model + epsilon)
    scale = scales[:, :1]
    gate = columns(0, width) * scale
    up = columns(padded, padded + width) * scale
    out[...] = (gate / (1.0 + jnp.exp(-gate)) * up).astype(bf16)


def scatter_rounds(keep, send, rows, tp, tail=True):
    width = keep.shape[1]
    acc, recvs = keep, [swap(send, "tp", tp, 1)]
    for shift, radix in digits_of(tp, 1)[1:]:
        n_out = acc.shape[0] // radix
        outs = [sds((n_out, width), f32)] + [sds((n_out, width), bf16)] * (radix - 1)
        got = call(
            functools.partial(split_kernel, rows, shift, radix, len(recvs), int(tail)),
            [acc, *recvs],
            outs,
        )
        acc = got[0]
        recvs = [swap(s, "tp", tp, k << shift) for k, s in enumerate(got[1:], 1)]
    return acc, recvs


def gather_rounds(x, tp):
    masks = [0]
    for shift, radix in digits_of(tp, 1)[1:]:
        x = jnp.concatenate([x] + [swap(x, "tp", tp, k << shift) for k in range(1, radix)], axis=0)
        masks = [m | (k << shift) for k in range(radix) for m in masks]
    return x, swap(x, "tp", tp, 1), masks


def sum_terms(part, kv):
    digits = digits_of(kv)
    terms = [part]
    for i, (shift, radix) in enumerate(digits):
        if i:
            part = tree([t.astype(f32) for t in terms]).astype(bf16)
        terms = [part] + [swap(part, "kv", kv, k << shift) for k in range(1, radix)]
    return terms


def solution(mesh):
    tp, kv = mesh.shape["tp"], mesh.shape["kv"]

    def body(
        tokens,
        norm_gain,
        query_weight,
        key_weight,
        value_weight,
        input_gate_weight,
        forget_gate_weight,
        input_gate_bias,
        forget_gate_bias,
        memory_state,
        normalizer_state,
        stabilizer_state,
        block_keys,
        block_values,
        block_input_pre,
        block_forget_pre,
        block_lengths,
        head_norm_gain,
        output_weight,
        mixer_norm_gain,
        gate_weight,
        up_weight,
        down_weight,
    ):
        total, depth = tokens.shape
        seqs, heads, block, size = block_keys.shape
        width = heads * size
        model = depth * tp
        all_heads = input_gate_weight.shape[1]
        half = total // 2
        bias_i, bias_f = input_gate_bias[None, :], forget_gate_bias[None, :]

        packed = 3 * width + LANES
        keep, send = call(
            functools.partial(project_kernel, seqs),
            [
                tokens,
                norm_gain[None, :],
                query_weight,
                key_weight,
                value_weight,
                input_gate_weight.T,
                forget_gate_weight.T,
            ],
            [sds((half, packed), f32), sds((half, packed), bf16)],
            [
                sds((total, depth), bf16),
                sds((1, depth), f32),
                *[sds((depth, width), bf16)] * 3,
                *[sds((all_heads, depth), bf16)] * 2,
                sds((total, depth), bf16),
            ],
            fetched=range(7),
            copies=7,
        )
        acc, recvs = scatter_rounds(keep, send, seqs, tp)
        prepared = call(
            gating_kernel,
            [
                block_input_pre,
                block_forget_pre,
                block_lengths[None, :],
                stabilizer_state.T,
                bias_i,
                bias_f,
                normalizer_state,
                head_norm_gain[None, :],
                block_keys,
                block_values,
                memory_state,
            ],
            [
                *[sds((heads * seqs, block), f32)] * 3,
                sds(block_keys.shape, bf16),
                sds(block_values.shape, bf16),
                sds((seqs, heads, 2 * size, size), bf16),
                sds(normalizer_state.shape, f32),
                sds((1, width), f32),
                sds((8, LANES), f32),
            ],
            [
                *[sds((seqs, heads, block), f32)] * 2,
                sds((1, seqs), jnp.int32),
                sds((heads, seqs), f32),
                *[sds((1, heads), f32)] * 2,
                sds(memory_state.shape, f32),
            ],
            fetched=range(11),
            copies=10 + PIECES,
        )
        (head_out,) = call(
            functools.partial(cell_kernel, (float(model), all_heads), len(recvs)),
            [acc, *recvs, *prepared],
            [sds((seqs, width), bf16)],
        )
        near, far, masks = gather_rounds(head_out, tp)
        (part,) = call(
            functools.partial(apply_kernel, masks, seqs),
            [near, far, output_weight],
            [sds((total, depth), bf16)],
            [sds((total, width), bf16)],
        )
        terms = sum_terms(part, kv)

        hidden_dev = gate_weight.shape[1]
        first = pl.cdiv(pl.cdiv(hidden_dev, LANES), 2) * LANES
        pieces = [(0, min(first, hidden_dev))]
        if hidden_dev > first:
            pieces.append((first, hidden_dev - first))
        packed = [2 * pl.cdiv(w, LANES) * LANES for _, w in pieces]
        packed[0] += LANES
        res, scaled, *split = call(
            functools.partial(mixer_kernel, seqs, pieces[0][1], len(terms)),
            [*terms, tokens, mixer_norm_gain[None, :], gate_weight, up_weight],
            [
                sds((total, depth), f32),
                sds((total, depth), bf16),
                sds((half, packed[0]), f32),
                sds((half, packed[0]), bf16),
            ],
            [sds((total, depth), f32)],
        )
        scales = part = None
        for i, (at, w) in enumerate(pieces):
            if i:
                split = call(
                    functools.partial(rest_kernel, at, w),
                    [scaled, gate_weight, up_weight],
                    [sds((half, packed[i]), f32), sds((half, packed[i]), bf16)],
                )
            acc, recvs = scatter_rounds(*split, seqs, tp, i == 0)
            got = call(
                functools.partial(activate_kernel, float(model), len(recvs), i == 0),
                [acc, *recvs] + ([scales] if i else []),
                [sds((seqs, w), bf16)] + ([] if i else [sds((seqs, LANES), f32)]),
            )
            if i == 0:
                scales = got[1]
            near, far, masks = gather_rounds(got[0], tp)
            last = i == len(pieces) - 1
            (part,) = call(
                functools.partial(down_kernel, masks, seqs, at, i > 0),
                [near, far, down_weight] + ([part] if i else []),
                [sds((total, depth), bf16 if last else f32)],
                [sds((total, w), bf16)],
            )
        terms = sum_terms(part, kv)
        return res + tree([t.astype(f32) for t in terms])

    placed = (
        P(None, "tp"),
        P("tp"),
        P("tp", "kv"),
        P("tp", "kv"),
        P("tp", "kv"),
        P("tp", None),
        P("tp", None),
        P("kv"),
        P("kv"),
        P("tp", "kv", None, None),
        P("tp", "kv", None),
        P("tp", "kv"),
        P("tp", "kv", None, None),
        P("tp", "kv", None, None),
        P("tp", "kv", None),
        P("tp", "kv", None),
        P("tp"),
        P("kv"),
        P("kv", "tp"),
        P("tp"),
        P("tp", "kv"),
        P("tp", "kv"),
        P("kv", "tp"),
    )
    return jax.shard_map(body, mesh=mesh, in_specs=placed, out_specs=P(None, "tp"), check_vma=False)
```

```python
import functools

import jax
import jax.numpy as jnp
from jax import lax
from jax.experimental import pallas as pl
from jax.experimental.pallas import tpu as pltpu
from jax.sharding import PartitionSpec as P


f32 = jnp.float32
bf16 = jnp.bfloat16
epsilon = 1e-06
LANES = 128
HALVES = 2
SCATTER_ORDER = {2: (1,), 4: (2, 1, 3)}
SMALL_ORDER = {2: (1,), 4: (1, 2, 3)}
LARGE_ORDER = {2: (1,), 4: (3, 1, 2)}
VMEM = pl.BlockSpec(memory_space=pltpu.VMEM)
HBM = pl.BlockSpec(memory_space=pltpu.HBM)


def size_of(x):
    n = x.dtype.itemsize
    for extent in x.shape:
        n *= extent
    return n


def call(kernel, ins, outs, scratch=(), flops=1, fetched=(), copies=0):
    total = sum(size_of(x) for x in ins) + sum(size_of(x) for x in outs)
    total += sum(size_of(x) for x in scratch)
    shapes = [pltpu.VMEM(s.shape, s.dtype) for s in scratch]
    if copies:
        shapes.append(pltpu.SemaphoreType.DMA((copies,)))
    return pl.pallas_call(
        kernel,
        out_shape=list(outs),
        in_specs=[HBM if i in fetched else VMEM for i in range(len(ins))],
        out_specs=[VMEM] * len(outs),
        scratch_shapes=shapes,
        compiler_params=pltpu.CompilerParams(vmem_limit_bytes=min(total + total // 4 + (6 << 20), 60 << 20)),
        cost_estimate=pl.CostEstimate(flops=flops, bytes_accessed=total, transcendentals=0),
    )(*[pinned(x) if i in fetched else x for i, x in enumerate(ins)])


def pinned(x):
    return pltpu.with_memory_space_constraint(x, pltpu.HBM) if x.size > 1 else x


def start_copies(pairs, sems):
    copies = [pltpu.make_async_copy(a, b, sems.at[i]) for i, (a, b) in enumerate(pairs)]
    for c in copies:
        c.start()
    return copies


def sds(shape, dtype):
    return jax.ShapeDtypeStruct(shape, dtype)


def digits_of(n, first=2):
    out, shift = [], 0
    left = n
    while left > 1:
        radix = min(2 if shift == 0 and first == 1 else 4, left)
        assert left % radix == 0 and radix in (2, 4)
        out.append((shift, radix))
        shift += radix.bit_length() - 1
        left //= radix
    return out


def swap(x, axis, n, mask):
    return lax.ppermute(x, axis, [(i, i ^ mask) for i in range(n)])


def digit_index(axis, shift, radix):
    return lax.rem(lax.div(lax.axis_index(axis), jnp.int32(1 << shift)), jnp.int32(radix))


def rows_at(index, rows):
    return pl.ds(pl.multiple_of(index * rows, rows), rows)


def join_tail(tail):
    return tail + pltpu.roll(tail, LANES // 2, 1)


def split_tail(both):
    lane = lax.broadcasted_iota(jnp.int32, both.shape, 1)
    high = both.astype(bf16).astype(f32)
    return jnp.where(lane < LANES // 2, high, both - high).astype(bf16)


def keep_tail(both):
    lane = lax.broadcasted_iota(jnp.int32, both.shape, 1)
    return jnp.where(lane < LANES // 2, both, 0.0)


def project_kernel(rows, *refs):
    hbm, (keep, send), local = refs[:7], refs[7:9], refs[9:16]
    perm, sems = refs[16:]
    copies = start_copies(list(zip(hbm, local)), sems)
    tok, gain, wq, wk, wv, wi, wf = local
    total = tok.shape[0]
    half = total // 2
    width = wq.shape[1]
    core = digit_index("tp", 0, 2)
    copies[0].wait()
    copies[1].wait()
    for z in range(half // rows):
        perm[z * rows : (z + 1) * rows, :] = tok[rows_at(2 * z + core, rows), :]
        perm[half + z * rows : half + (z + 1) * rows, :] = tok[rows_at(2 * z + 1 - core, rows), :]
    wide = perm[...].astype(f32)
    scaled = (wide * gain[...]).astype(bf16)
    squares = jnp.sum(wide * wide, axis=1, keepdims=True)
    for i, w in enumerate((wq, wk, wv)):
        copies[2 + i].wait()
        p = jnp.dot(scaled, w[...], preferred_element_type=f32)
        keep[:, i * width : (i + 1) * width] = p[:half]
        send[:, i * width : (i + 1) * width] = p[half:].astype(bf16)
    copies[5].wait()
    copies[6].wait()
    gates = [
        lax.dot_general(scaled, w[...], (((1,), (1,)), ((), ())), preferred_element_type=f32)
        for w in (wi, wf)
    ]
    blank = jnp.zeros((total, LANES // 2 - 2 * wi.shape[0] - 1), f32)
    tail = jnp.concatenate([*gates, squares, blank] * 2, axis=1)
    keep[:, 3 * width :] = keep_tail(tail[:half])
    send[:, 3 * width :] = split_tail(tail[half:])


def split_kernel(rows, shift, radix, n_recv, tail, *refs):
    acc, recvs = refs[0], refs[1 : 1 + n_recv]
    mine, sends = refs[1 + n_recv], refs[2 + n_recv :]
    body = acc.shape[1] - LANES * tail
    digit = digit_index("tp", shift, radix)
    for block in range(acc.shape[0] // (radix * rows)):
        to = slice(block * rows, (block + 1) * rows)
        for i, k in enumerate((0, *SCATTER_ORDER[radix])):
            at = rows_at(block * radix + (digit ^ k), rows)
            value = acc[at, :]
            for r in recvs:
                value = value + r[at, :].astype(f32)
            if k == 0:
                mine[to, :] = value
            else:
                sends[i - 1][to, :body] = value[:, :body].astype(bf16)
                if tail:
                    sends[i - 1][to, body:] = split_tail(join_tail(value[:, body:]))


def row_to_column(values, seqs):
    row = lax.broadcasted_iota(jnp.int32, (seqs, seqs), 0)
    lane = lax.broadcasted_iota(jnp.int32, (seqs, seqs), 1)
    return jnp.sum(jnp.where(row == lane, values, 0.0), axis=1, keepdims=True)


def gating_kernel(*refs):
    small, (keys_in, values_in, memory_in) = refs[:8], refs[8:11]
    e0, carried, top, keys, values, memory, normalizer, gain, biases = refs[11:20]
    local, sems = refs[20:26], refs[26]
    ipre, fpre, lens, stab, bias_i, bias_f = local
    seqs, heads, block = ipre.shape
    pairs = list(zip(small, (*local, normalizer, gain)))
    pairs += [(memory_in, memory), (keys_in, keys), (values_in, values)]
    copies = start_copies(pairs, sems)
    for c in copies[:6]:
        c.wait()
    biases[0:1, :heads] = bias_i[...]
    biases[1:2, :heads] = bias_f[...]
    length = row_to_column(lens[...].astype(f32), seqs)
    position = lax.broadcasted_iota(jnp.int32, (seqs, block), 1).astype(f32)
    live = position < length
    before = lax.broadcasted_iota(jnp.int32, (block, block), 0)
    after = lax.broadcasted_iota(jnp.int32, (block, block), 1)
    mask = (before > after).astype(f32)
    for h in range(heads):
        to = slice(h * seqs, (h + 1) * seqs)
        pre = fpre[:, h, :] + bias_f[:, h : h + 1]
        log_sig = jnp.minimum(pre, 0.0) - jnp.log1p(jnp.exp(-jnp.abs(pre)))
        forget = jnp.where(live, log_sig, 0.0)
        later = jnp.dot(forget, mask, precision=lax.Precision.HIGHEST, preferred_element_type=f32)
        exponent = jnp.where(live, later + (ipre[:, h, :] + bias_i[:, h : h + 1]), -jnp.inf)
        state = jnp.sum(forget, axis=1, keepdims=True) + row_to_column(stab[h : h + 1, :], seqs)
        e0[to, :] = exponent
        carried[to, :] = jnp.broadcast_to(state, exponent.shape)
        largest = jnp.maximum(jnp.max(exponent, axis=1, keepdims=True), state)
        top[to, :] = jnp.broadcast_to(largest, exponent.shape)
    for c in copies[6:]:
        c.wait()


def cell_kernel(model, n_recv, *refs):
    acc, recvs = refs[0], refs[1 : 1 + n_recv]
    e0, carried, top, keys, values, memory, normalizer, gain, biases, out = refs[1 + n_recv :]
    seqs, heads, size = normalizer.shape
    width = heads * size
    all_heads = model[1]

    def columns(start, stop):
        value = acc[:, start:stop]
        for r in recvs:
            value = value + r[:, start:stop].astype(f32)
        return value

    tail = join_tail(columns(3 * width, 3 * width + LANES))
    lane = lax.broadcasted_iota(jnp.int32, tail.shape, 1)

    def pick(at):
        return jnp.sum(jnp.where(lane == at, tail, 0.0), axis=1, keepdims=True)

    scale = lax.rsqrt(tail[:, 2 * all_heads : 2 * all_heads + 1] / model[0] + epsilon)
    first = lax.axis_index("kv") * heads
    row = lax.broadcasted_iota(jnp.int32, (seqs, size), 0)
    for h in range(heads):
        at = slice(h * size, (h + 1) * size)
        to = slice(h * seqs, (h + 1) * seqs)
        in_lane = first + h
        log_input = pick(in_lane) * scale + biases[0:1, h : h + 1]
        pre = pick(in_lane + all_heads) * scale + biases[1:2, h : h + 1]
        log_forget = jnp.minimum(pre, 0.0) - jnp.log1p(jnp.exp(-jnp.abs(pre)))
        stab_max = jnp.maximum(top[to, :] + log_forget, log_input)
        query = (columns(at.start, at.stop) * scale * size ** (-0.5)).astype(bf16)
        new_key = (columns(width + at.start, width + at.stop) * scale).astype(bf16).astype(f32)
        new_value = (columns(2 * width + at.start, 2 * width + at.stop) * scale).astype(bf16).astype(f32)
        wide = query.astype(f32)
        upright = wide.T
        scores = jnp.zeros((seqs, size), f32)
        state_sum = jnp.zeros((seqs, size), f32)
        for b in range(seqs):
            s = lax.dot_general(query, keys[b, h], (((1,), (1,)), ((), ())), preferred_element_type=f32)
            scores = jnp.where(row == b, s, scores)
            m = jnp.sum(memory[b, h] * upright[:, b : b + 1], axis=0, keepdims=True)
            state_sum = jnp.where(row == b, m, state_sum)
        weight = jnp.exp(e0[to, :] + log_forget - stab_max) * scores
        probs = weight.astype(bf16)
        block_sum = jnp.zeros((seqs, size), f32)
        for b in range(seqs):
            p = jnp.dot(probs, values[b, h], preferred_element_type=f32)
            block_sum = jnp.where(row == b, p, block_sum)
        new_weight = jnp.exp(log_input - stab_max) * jnp.sum(wide * new_key, axis=1, keepdims=True)
        state_weight = jnp.exp(carried[to, :] + log_forget - stab_max)
        state_norm = jnp.sum(normalizer[:, h, :] * wide, axis=1, keepdims=True)
        numerator = block_sum + new_weight * new_value + state_weight * state_sum
        denominator = jnp.sum(weight, axis=1, keepdims=True) + new_weight + state_weight * state_norm
        cell = numerator / jnp.maximum(jnp.abs(denominator), 1.0)
        out[:, at] = (cell * gain[:, at]).astype(bf16)


def place_rows(masks, rows, near, far, whole):
    me = lax.axis_index("tp")
    for part, core in ((near, 0), (far, 1)):
        for i, mask in enumerate(masks):
            whole[rows_at(me ^ (mask | core), rows), :] = part[i * rows : (i + 1) * rows, :]


def apply_kernel(masks, rows, near, far, w, out, whole):
    place_rows(masks, rows, near, far, whole)
    out[...] = jnp.dot(whole[...], w[...], preferred_element_type=f32).astype(bf16)


def down_kernel(masks, rows, at, more, *refs):
    near, far, w = refs[:3]
    out, whole = refs[-2:]
    place_rows(masks, rows, near, far, whole)
    width = near.shape[1]
    value = jnp.dot(whole[...], w[at : at + width, :], preferred_element_type=f32)
    if more:
        value = value + refs[3][...]
    out[...] = value.astype(out.dtype)


def tree(values):
    while len(values) > 1:
        values = [a + b for a, b in zip(values[::2], values[1::2])]
    return values[0]


def write_products(scaled, weights, at, width, keep, send):
    half = keep.shape[0]
    padded = pl.cdiv(width, LANES) * LANES
    for i, w in enumerate(weights):
        for start in range(0, width, 512):
            stop = min(start + 512, width)
            p = jnp.dot(scaled, w[:, at + start : at + stop], preferred_element_type=f32)
            keep[:, i * padded + start : i * padded + stop] = p[:half]
            send[:, i * padded + start : i * padded + stop] = p[half:].astype(bf16)


def mixer_kernel(rows, width, n_terms, *refs):
    terms = refs[:n_terms]
    tok, gain, wg, wu, res, scaled, keep, send, perm = refs[n_terms:]
    total = tok.shape[0]
    half = total // 2
    core = digit_index("tp", 0, 2)
    res[...] = tok[...].astype(f32) + tree([t[...].astype(f32) for t in terms])
    for z in range(half // rows):
        perm[z * rows : (z + 1) * rows, :] = res[rows_at(2 * z + core, rows), :]
        perm[half + z * rows : half + (z + 1) * rows, :] = res[rows_at(2 * z + 1 - core, rows), :]
    wide = perm[...]
    squares = jnp.broadcast_to(jnp.sum(wide * wide, axis=1, keepdims=True), (total, LANES))
    keep[:, keep.shape[1] - LANES :] = keep_tail(squares[:half])
    send[:, keep.shape[1] - LANES :] = split_tail(squares[half:])
    scaled[...] = (wide * gain[...]).astype(bf16)
    write_products(scaled[...], (wg, wu), 0, width, keep, send)


def rest_kernel(at, width, scaled, wg, wu, keep, send):
    write_products(scaled[...], (wg, wu), at, width, keep, send)


def pack(value, tail, send, to):
    body = value.shape[1] - LANES * tail
    send[to, :body] = value[:, :body].astype(bf16)
    if tail:
        send[to, body:] = split_tail(join_tail(value[:, body:]))


def first_half_kernel(rows, shift, order, n_recv, tail, *refs):
    acc, recvs = refs[0], refs[1 : 1 + n_recv]
    keep, send = refs[1 + n_recv :]
    digit = digit_index("tp", shift, 4)
    p, q = order
    blocks = acc.shape[0] // (4 * rows)
    for block in range(blocks):
        for half, (first, second) in enumerate(((0, p), (q, p ^ q))):
            to = slice((half * blocks + block) * rows, (half * blocks + block + 1) * rows)
            for mask in (second, first):
                at = rows_at(block * 4 + (digit ^ mask), rows)
                value = acc[at, :]
                for r in recvs:
                    value = value + r[at, :].astype(f32)
                if mask == first:
                    keep[to, :] = value
                else:
                    pack(value, tail, send, to)


def second_half_kernel(tail, acc, recv, mine, send):
    half = acc.shape[0] // 2
    pack(acc[half:, :] + recv[half:, :].astype(f32), tail, send, slice(0, half))
    mine[...] = acc[:half, :] + recv[:half, :].astype(f32)


def activate_kernel(model, n_recv, first, *refs):
    acc, recvs = refs[0], refs[1 : 1 + n_recv]
    if first:
        out, scales = refs[-2:]
    else:
        scales, out = refs[-2:]
    width = out.shape[1]
    padded = pl.cdiv(width, LANES) * LANES

    def columns(start, stop):
        value = acc[:, start:stop]
        for r in recvs:
            value = value + r[:, start:stop].astype(f32)
        return value

    if first:
        tail = join_tail(columns(2 * padded, 2 * padded + LANES))
        scales[...] = lax.rsqrt(tail / model + epsilon)
    scale = scales[:, :1]
    gate = columns(0, width) * scale
    up = columns(padded, padded + width) * scale
    out[...] = (gate / (1.0 + jnp.exp(-gate)) * up).astype(bf16)


def scatter_rounds(keep, send, rows, tp, tail=True):
    width = keep.shape[1]
    acc, recvs = keep, [swap(send, "tp", tp, 1)]
    for shift, radix in digits_of(tp, 1)[1:]:
        n_out = acc.shape[0] // radix
        outs = [sds((n_out, width), f32)] + [sds((n_out, width), bf16)] * (radix - 1)
        got = call(
            functools.partial(split_kernel, rows, shift, radix, len(recvs), int(tail)),
            [acc, *recvs],
            outs,
        )
        acc = got[0]
        recvs = [swap(s, "tp", tp, k << shift) for k, s in zip(SCATTER_ORDER[radix], got[1:])]
    return acc, recvs


def paired_scatter_rounds(keep, send, rows, tp, order, tail):
    width = keep.shape[1]
    acc, recvs = keep, [swap(send, "tp", tp, 1)]
    for shift, radix in digits_of(tp, 1)[1:]:
        n = acc.shape[0]
        if radix != 4:
            acc, out = call(
                functools.partial(split_kernel, rows, shift, radix, len(recvs), int(tail)),
                [acc, *recvs],
                [sds((n // radix, width), f32), sds((n // radix, width), bf16)],
            )
            recvs = [swap(out, "tp", tp, 1 << shift)]
            continue
        acc, out = call(
            functools.partial(first_half_kernel, rows, shift, order, len(recvs), int(tail)),
            [acc, *recvs],
            [sds((n // 2, width), f32), sds((n // 2, width), bf16)],
        )
        recv = swap(out, "tp", tp, order[0] << shift)
        acc, out = call(
            functools.partial(second_half_kernel, int(tail)),
            [acc, recv],
            [sds((n // 4, width), f32), sds((n // 4, width), bf16)],
        )
        recvs = [swap(out, "tp", tp, order[1] << shift)]
    return acc, recvs


def gather_rounds(x, tp, orders):
    masks = [0]
    for shift, radix in digits_of(tp, 1)[1:]:
        order = orders[radix]
        x = jnp.concatenate([x] + [swap(x, "tp", tp, k << shift) for k in order], axis=0)
        masks = [m | (k << shift) for k in (0, *order) for m in masks]
    return x, swap(x, "tp", tp, 1), masks


def sum_terms(part, kv):
    digits = digits_of(kv)
    terms = [part]
    for i, (shift, radix) in enumerate(digits):
        if i:
            part = tree([t.astype(f32) for t in terms]).astype(bf16)
        terms = [part] + [swap(part, "kv", kv, k << shift) for k in range(1, radix)]
    return terms


def solution(mesh):
    tp, kv = mesh.shape["tp"], mesh.shape["kv"]

    def body(
        tokens,
        norm_gain,
        query_weight,
        key_weight,
        value_weight,
        input_gate_weight,
        forget_gate_weight,
        input_gate_bias,
        forget_gate_bias,
        memory_state,
        normalizer_state,
        stabilizer_state,
        block_keys,
        block_values,
        block_input_pre,
        block_forget_pre,
        block_lengths,
        head_norm_gain,
        output_weight,
        mixer_norm_gain,
        gate_weight,
        up_weight,
        down_weight,
    ):
        total, depth = tokens.shape
        seqs, heads, block, size = block_keys.shape
        width = heads * size
        model = depth * tp
        all_heads = input_gate_weight.shape[1]
        half = total // 2
        bias_i, bias_f = input_gate_bias[None, :], forget_gate_bias[None, :]

        packed = 3 * width + LANES
        keep, send = call(
            functools.partial(project_kernel, seqs),
            [
                tokens,
                norm_gain[None, :],
                query_weight,
                key_weight,
                value_weight,
                input_gate_weight.T,
                forget_gate_weight.T,
            ],
            [sds((half, packed), f32), sds((half, packed), bf16)],
            [
                sds((total, depth), bf16),
                sds((1, depth), f32),
                *[sds((depth, width), bf16)] * 3,
                *[sds((all_heads, depth), bf16)] * 2,
                sds((total, depth), bf16),
            ],
            fetched=range(7),
            copies=7,
        )
        acc, recvs = scatter_rounds(keep, send, seqs, tp)
        prepared = call(
            gating_kernel,
            [
                block_input_pre,
                block_forget_pre,
                block_lengths[None, :],
                stabilizer_state.T,
                bias_i,
                bias_f,
                normalizer_state,
                head_norm_gain[None, :],
                block_keys,
                block_values,
                memory_state,
            ],
            [
                *[sds((heads * seqs, block), f32)] * 3,
                sds(block_keys.shape, bf16),
                sds(block_values.shape, bf16),
                sds(memory_state.shape, f32),
                sds(normalizer_state.shape, f32),
                sds((1, width), f32),
                sds((8, LANES), f32),
            ],
            [
                *[sds((seqs, heads, block), f32)] * 2,
                sds((1, seqs), jnp.int32),
                sds((heads, seqs), f32),
                *[sds((1, heads), f32)] * 2,
            ],
            fetched=range(11),
            copies=11,
        )
        (head_out,) = call(
            functools.partial(cell_kernel, (float(model), all_heads), len(recvs)),
            [acc, *recvs, *prepared],
            [sds((seqs, width), bf16)],
        )
        near, far, masks = gather_rounds(head_out, tp, SMALL_ORDER)
        (part,) = call(
            functools.partial(apply_kernel, masks, seqs),
            [near, far, output_weight],
            [sds((total, depth), bf16)],
            [sds((total, width), bf16)],
        )
        terms = sum_terms(part, kv)

        hidden_dev = gate_weight.shape[1]
        first = pl.cdiv(pl.cdiv(hidden_dev, LANES), HALVES) * LANES
        pieces = [(0, min(first, hidden_dev))]
        if hidden_dev > first:
            pieces.append((first, hidden_dev - first))
        packed = [2 * pl.cdiv(w, LANES) * LANES for _, w in pieces]
        packed[0] += LANES
        res, scaled, *split = call(
            functools.partial(mixer_kernel, seqs, pieces[0][1], len(terms)),
            [*terms, tokens, mixer_norm_gain[None, :], gate_weight, up_weight],
            [
                sds((total, depth), f32),
                sds((total, depth), bf16),
                sds((half, packed[0]), f32),
                sds((half, packed[0]), bf16),
            ],
            [sds((total, depth), f32)],
        )
        scales = part = None
        for i, (at, w) in enumerate(pieces):
            if i:
                split = call(
                    functools.partial(rest_kernel, at, w),
                    [scaled, gate_weight, up_weight],
                    [sds((half, packed[i]), f32), sds((half, packed[i]), bf16)],
                )
            acc, recvs = paired_scatter_rounds(*split, seqs, tp, ((1, 3), (3, 1))[i], i == 0)
            got = call(
                functools.partial(activate_kernel, float(model), len(recvs), i == 0),
                [acc, *recvs] + ([scales] if i else []),
                [sds((seqs, w), bf16)] + ([] if i else [sds((seqs, LANES), f32)]),
            )
            if i == 0:
                scales = got[1]
            near, far, masks = gather_rounds(got[0], tp, LARGE_ORDER)
            last = i == len(pieces) - 1
            (part,) = call(
                functools.partial(down_kernel, masks, seqs, at, i > 0),
                [near, far, down_weight] + ([part] if i else []),
                [sds((total, depth), bf16 if last else f32)],
                [sds((total, w), bf16)],
            )
        terms = sum_terms(part, kv)
        return res + tree([t.astype(f32) for t in terms])

    placed = (
        P(None, "tp"),
        P("tp"),
        P("tp", "kv"),
        P("tp", "kv"),
        P("tp", "kv"),
        P("tp", None),
        P("tp", None),
        P("kv"),
        P("kv"),
        P("tp", "kv", None, None),
        P("tp", "kv", None),
        P("tp", "kv"),
        P("tp", "kv", None, None),
        P("tp", "kv", None, None),
        P("tp", "kv", None),
        P("tp", "kv", None),
        P("tp"),
        P("kv"),
        P("kv", "tp"),
        P("tp"),
        P("tp", "kv"),
        P("tp", "kv"),
        P("kv", "tp"),
    )
    return jax.shard_map(body, mesh=mesh, in_specs=placed, out_specs=P(None, "tp"), check_vma=False)
```

```python
import functools

import jax
import jax.numpy as jnp
from jax import lax
from jax.experimental import pallas as pl
from jax.experimental.pallas import tpu as pltpu
from jax.sharding import PartitionSpec as P


f32 = jnp.float32
bf16 = jnp.bfloat16
epsilon = 1e-06
LANES = 128
HALVES = 2
SCATTER_ORDER = {2: (1,), 4: (2, 1, 3)}
SMALL_ORDER = {2: (1,), 4: (1, 2, 3)}
LARGE_ORDER = {2: (1,), 4: (1, 2, 3)}
VMEM = pl.BlockSpec(memory_space=pltpu.VMEM)
HBM = pl.BlockSpec(memory_space=pltpu.HBM)


def size_of(x):
    n = x.dtype.itemsize
    for extent in x.shape:
        n *= extent
    return n


def call(kernel, ins, outs, scratch=(), flops=1, fetched=(), copies=0):
    total = sum(size_of(x) for x in ins) + sum(size_of(x) for x in outs)
    total += sum(size_of(x) for x in scratch)
    shapes = [pltpu.VMEM(s.shape, s.dtype) for s in scratch]
    if copies:
        shapes.append(pltpu.SemaphoreType.DMA((copies,)))
    return pl.pallas_call(
        kernel,
        out_shape=list(outs),
        in_specs=[HBM if i in fetched else VMEM for i in range(len(ins))],
        out_specs=[VMEM] * len(outs),
        scratch_shapes=shapes,
        compiler_params=pltpu.CompilerParams(vmem_limit_bytes=min(total + total // 4 + (6 << 20), 60 << 20)),
        cost_estimate=pl.CostEstimate(flops=flops, bytes_accessed=total, transcendentals=0),
    )(*[pinned(x) if i in fetched else x for i, x in enumerate(ins)])


def pinned(x):
    return pltpu.with_memory_space_constraint(x, pltpu.HBM) if x.size > 1 else x


def start_copies(pairs, sems):
    copies = [pltpu.make_async_copy(a, b, sems.at[i]) for i, (a, b) in enumerate(pairs)]
    for c in copies:
        c.start()
    return copies


def sds(shape, dtype):
    return jax.ShapeDtypeStruct(shape, dtype)


def digits_of(n, first=2):
    out, shift = [], 0
    left = n
    while left > 1:
        radix = min(2 if shift == 0 and first == 1 else 4, left)
        assert left % radix == 0 and radix in (2, 4)
        out.append((shift, radix))
        shift += radix.bit_length() - 1
        left //= radix
    return out


def swap(x, axis, n, mask):
    return lax.ppermute(x, axis, [(i, i ^ mask) for i in range(n)])


def digit_index(axis, shift, radix):
    return lax.rem(lax.div(lax.axis_index(axis), jnp.int32(1 << shift)), jnp.int32(radix))


def rows_at(index, rows):
    return pl.ds(pl.multiple_of(index * rows, rows), rows)


def join_tail(tail):
    return tail + pltpu.roll(tail, LANES // 2, 1)


def split_tail(both):
    lane = lax.broadcasted_iota(jnp.int32, both.shape, 1)
    high = both.astype(bf16).astype(f32)
    return jnp.where(lane < LANES // 2, high, both - high).astype(bf16)


def keep_tail(both):
    lane = lax.broadcasted_iota(jnp.int32, both.shape, 1)
    return jnp.where(lane < LANES // 2, both, 0.0)


def project_kernel(rows, *refs):
    hbm, (keep, send), local = refs[:7], refs[7:9], refs[9:16]
    perm, sems = refs[16:]
    copies = start_copies(list(zip(hbm, local)), sems)
    tok, gain, wq, wk, wv, wi, wf = local
    total = tok.shape[0]
    half = total // 2
    width = wq.shape[1]
    core = digit_index("tp", 0, 2)
    copies[0].wait()
    copies[1].wait()
    for z in range(half // rows):
        perm[z * rows : (z + 1) * rows, :] = tok[rows_at(2 * z + core, rows), :]
        perm[half + z * rows : half + (z + 1) * rows, :] = tok[rows_at(2 * z + 1 - core, rows), :]
    wide = perm[...].astype(f32)
    scaled = (wide * gain[...]).astype(bf16)
    squares = jnp.sum(wide * wide, axis=1, keepdims=True)
    for i, w in enumerate((wq, wk, wv)):
        copies[2 + i].wait()
        p = jnp.dot(scaled, w[...], preferred_element_type=f32)
        keep[:, i * width : (i + 1) * width] = p[:half]
        send[:, i * width : (i + 1) * width] = p[half:].astype(bf16)
    copies[5].wait()
    copies[6].wait()
    gates = [
        lax.dot_general(scaled, w[...], (((1,), (1,)), ((), ())), preferred_element_type=f32)
        for w in (wi, wf)
    ]
    blank = jnp.zeros((total, LANES // 2 - 2 * wi.shape[0] - 1), f32)
    tail = jnp.concatenate([*gates, squares, blank] * 2, axis=1)
    keep[:, 3 * width :] = keep_tail(tail[:half])
    send[:, 3 * width :] = split_tail(tail[half:])


def split_kernel(rows, shift, radix, n_recv, tail, *refs):
    acc, recvs = refs[0], refs[1 : 1 + n_recv]
    mine, sends = refs[1 + n_recv], refs[2 + n_recv :]
    body = acc.shape[1] - LANES * tail
    digit = digit_index("tp", shift, radix)
    for block in range(acc.shape[0] // (radix * rows)):
        to = slice(block * rows, (block + 1) * rows)
        for i, k in enumerate((0, *SCATTER_ORDER[radix])):
            at = rows_at(block * radix + (digit ^ k), rows)
            value = acc[at, :]
            for r in recvs:
                value = value + r[at, :].astype(f32)
            if k == 0:
                mine[to, :] = value
            else:
                sends[i - 1][to, :body] = value[:, :body].astype(bf16)
                if tail:
                    sends[i - 1][to, body:] = split_tail(join_tail(value[:, body:]))


def row_to_column(values, seqs):
    row = lax.broadcasted_iota(jnp.int32, (seqs, seqs), 0)
    lane = lax.broadcasted_iota(jnp.int32, (seqs, seqs), 1)
    return jnp.sum(jnp.where(row == lane, values, 0.0), axis=1, keepdims=True)


def gating_kernel(*refs):
    small, (keys_in, values_in, memory_in) = refs[:8], refs[8:11]
    e0, carried, top, keys, values, memory, normalizer, gain, biases = refs[11:20]
    local, sems = refs[20:26], refs[26]
    ipre, fpre, lens, stab, bias_i, bias_f = local
    seqs, heads, block = ipre.shape
    pairs = list(zip(small, (*local, normalizer, gain)))
    pairs += [(memory_in, memory), (keys_in, keys), (values_in, values)]
    copies = start_copies(pairs, sems)
    for c in copies[:6]:
        c.wait()
    biases[0:1, :heads] = bias_i[...]
    biases[1:2, :heads] = bias_f[...]
    length = row_to_column(lens[...].astype(f32), seqs)
    position = lax.broadcasted_iota(jnp.int32, (seqs, block), 1).astype(f32)
    live = position < length
    before = lax.broadcasted_iota(jnp.int32, (block, block), 0)
    after = lax.broadcasted_iota(jnp.int32, (block, block), 1)
    mask = (before > after).astype(f32)
    for h in range(heads):
        to = slice(h * seqs, (h + 1) * seqs)
        pre = fpre[:, h, :] + bias_f[:, h : h + 1]
        log_sig = jnp.minimum(pre, 0.0) - jnp.log1p(jnp.exp(-jnp.abs(pre)))
        forget = jnp.where(live, log_sig, 0.0)
        later = jnp.dot(forget, mask, precision=lax.Precision.HIGHEST, preferred_element_type=f32)
        exponent = jnp.where(live, later + (ipre[:, h, :] + bias_i[:, h : h + 1]), -jnp.inf)
        state = jnp.sum(forget, axis=1, keepdims=True) + row_to_column(stab[h : h + 1, :], seqs)
        e0[to, :] = exponent
        carried[to, :] = jnp.broadcast_to(state, exponent.shape)
        largest = jnp.maximum(jnp.max(exponent, axis=1, keepdims=True), state)
        top[to, :] = jnp.broadcast_to(largest, exponent.shape)
    for c in copies[6:]:
        c.wait()


def cell_kernel(model, n_recv, *refs):
    acc, recvs = refs[0], refs[1 : 1 + n_recv]
    e0, carried, top, keys, values, memory, normalizer, gain, biases, out = refs[1 + n_recv :]
    seqs, heads, size = normalizer.shape
    width = heads * size
    all_heads = model[1]

    def columns(start, stop):
        value = acc[:, start:stop]
        for r in recvs:
            value = value + r[:, start:stop].astype(f32)
        return value

    tail = join_tail(columns(3 * width, 3 * width + LANES))
    lane = lax.broadcasted_iota(jnp.int32, tail.shape, 1)

    def pick(at):
        return jnp.sum(jnp.where(lane == at, tail, 0.0), axis=1, keepdims=True)

    scale = lax.rsqrt(tail[:, 2 * all_heads : 2 * all_heads + 1] / model[0] + epsilon)
    first = lax.axis_index("kv") * heads
    row = lax.broadcasted_iota(jnp.int32, (seqs, size), 0)
    for h in range(heads):
        at = slice(h * size, (h + 1) * size)
        to = slice(h * seqs, (h + 1) * seqs)
        in_lane = first + h
        log_input = pick(in_lane) * scale + biases[0:1, h : h + 1]
        pre = pick(in_lane + all_heads) * scale + biases[1:2, h : h + 1]
        log_forget = jnp.minimum(pre, 0.0) - jnp.log1p(jnp.exp(-jnp.abs(pre)))
        stab_max = jnp.maximum(top[to, :] + log_forget, log_input)
        query = (columns(at.start, at.stop) * scale * size ** (-0.5)).astype(bf16)
        new_key = (columns(width + at.start, width + at.stop) * scale).astype(bf16).astype(f32)
        new_value = (columns(2 * width + at.start, 2 * width + at.stop) * scale).astype(bf16).astype(f32)
        wide = query.astype(f32)
        upright = wide.T
        scores = jnp.zeros((seqs, size), f32)
        state_sum = jnp.zeros((seqs, size), f32)
        for b in range(seqs):
            s = lax.dot_general(query, keys[b, h], (((1,), (1,)), ((), ())), preferred_element_type=f32)
            scores = jnp.where(row == b, s, scores)
            m = jnp.sum(memory[b, h] * upright[:, b : b + 1], axis=0, keepdims=True)
            state_sum = jnp.where(row == b, m, state_sum)
        weight = jnp.exp(e0[to, :] + log_forget - stab_max) * scores
        probs = weight.astype(bf16)
        block_sum = jnp.zeros((seqs, size), f32)
        for b in range(seqs):
            p = jnp.dot(probs, values[b, h], preferred_element_type=f32)
            block_sum = jnp.where(row == b, p, block_sum)
        new_weight = jnp.exp(log_input - stab_max) * jnp.sum(wide * new_key, axis=1, keepdims=True)
        state_weight = jnp.exp(carried[to, :] + log_forget - stab_max)
        state_norm = jnp.sum(normalizer[:, h, :] * wide, axis=1, keepdims=True)
        numerator = block_sum + new_weight * new_value + state_weight * state_sum
        denominator = jnp.sum(weight, axis=1, keepdims=True) + new_weight + state_weight * state_norm
        cell = numerator / jnp.maximum(jnp.abs(denominator), 1.0)
        out[:, at] = (cell * gain[:, at]).astype(bf16)


def place_rows(masks, rows, near, far, whole):
    me = lax.axis_index("tp")
    for part, core in ((near, 0), (far, 1)):
        for i, mask in enumerate(masks):
            whole[rows_at(me ^ (mask | core), rows), :] = part[i * rows : (i + 1) * rows, :]


def apply_kernel(masks, rows, near, far, w, out, whole):
    place_rows(masks, rows, near, far, whole)
    out[...] = jnp.dot(whole[...], w[...], preferred_element_type=f32).astype(bf16)


def down_kernel(masks, rows, at, more, *refs):
    near, far, w = refs[:3]
    out, whole = refs[-2:]
    place_rows(masks, rows, near, far, whole)
    width = near.shape[1]
    value = jnp.dot(whole[...], w[at : at + width, :], preferred_element_type=f32)
    if more:
        value = value + refs[3][...]
    out[...] = value.astype(out.dtype)


def tree(values):
    while len(values) > 1:
        values = [a + b for a, b in zip(values[::2], values[1::2])]
    return values[0]


def write_products(scaled, weights, at, width, keep, send):
    half = keep.shape[0]
    padded = pl.cdiv(width, LANES) * LANES
    for i, w in enumerate(weights):
        for start in range(0, width, 512):
            stop = min(start + 512, width)
            p = jnp.dot(scaled, w[:, at + start : at + stop], preferred_element_type=f32)
            keep[:, i * padded + start : i * padded + stop] = p[:half]
            send[:, i * padded + start : i * padded + stop] = p[half:].astype(bf16)


def mixer_kernel(rows, width, n_terms, *refs):
    terms = refs[:n_terms]
    tok, gain, wg, wu, res, scaled, keep, send, perm = refs[n_terms:]
    total = tok.shape[0]
    half = total // 2
    core = digit_index("tp", 0, 2)
    res[...] = tok[...].astype(f32) + tree([t[...].astype(f32) for t in terms])
    for z in range(half // rows):
        perm[z * rows : (z + 1) * rows, :] = res[rows_at(2 * z + core, rows), :]
        perm[half + z * rows : half + (z + 1) * rows, :] = res[rows_at(2 * z + 1 - core, rows), :]
    wide = perm[...]
    squares = jnp.broadcast_to(jnp.sum(wide * wide, axis=1, keepdims=True), (total, LANES))
    keep[:, keep.shape[1] - LANES :] = keep_tail(squares[:half])
    send[:, keep.shape[1] - LANES :] = split_tail(squares[half:])
    scaled[...] = (wide * gain[...]).astype(bf16)
    write_products(scaled[...], (wg, wu), 0, width, keep, send)


def rest_kernel(at, width, scaled, wg, wu, keep, send):
    write_products(scaled[...], (wg, wu), at, width, keep, send)


def pack(value, tail, send, to):
    body = value.shape[1] - LANES * tail
    send[to, :body] = value[:, :body].astype(bf16)
    if tail:
        send[to, body:] = split_tail(join_tail(value[:, body:]))


def first_half_kernel(rows, shift, order, n_recv, tail, *refs):
    acc, recvs = refs[0], refs[1 : 1 + n_recv]
    keep, send = refs[1 + n_recv :]
    digit = digit_index("tp", shift, 4)
    p, q = order
    blocks = acc.shape[0] // (4 * rows)
    for block in range(blocks):
        for half, (first, second) in enumerate(((0, p), (q, p ^ q))):
            to = slice((half * blocks + block) * rows, (half * blocks + block + 1) * rows)
            for mask in (second, first):
                at = rows_at(block * 4 + (digit ^ mask), rows)
                value = acc[at, :]
                for r in recvs:
                    value = value + r[at, :].astype(f32)
                if mask == first:
                    keep[to, :] = value
                else:
                    pack(value, tail, send, to)


def second_half_kernel(tail, acc, recv, mine, send):
    half = acc.shape[0] // 2
    pack(acc[half:, :] + recv[half:, :].astype(f32), tail, send, slice(0, half))
    mine[...] = acc[:half, :] + recv[:half, :].astype(f32)


def activate_kernel(model, n_recv, first, *refs):
    acc, recvs = refs[0], refs[1 : 1 + n_recv]
    if first:
        out, scales = refs[-2:]
    else:
        scales, out = refs[-2:]
    width = out.shape[1]
    padded = pl.cdiv(width, LANES) * LANES

    def columns(start, stop):
        value = acc[:, start:stop]
        for r in recvs:
            value = value + r[:, start:stop].astype(f32)
        return value

    if first:
        tail = join_tail(columns(2 * padded, 2 * padded + LANES))
        scales[...] = lax.rsqrt(tail / model + epsilon)
    scale = scales[:, :1]
    gate = columns(0, width) * scale
    up = columns(padded, padded + width) * scale
    out[...] = (gate / (1.0 + jnp.exp(-gate)) * up).astype(bf16)


def scatter_rounds(keep, send, rows, tp, tail=True):
    width = keep.shape[1]
    acc, recvs = keep, [swap(send, "tp", tp, 1)]
    for shift, radix in digits_of(tp, 1)[1:]:
        n_out = acc.shape[0] // radix
        outs = [sds((n_out, width), f32)] + [sds((n_out, width), bf16)] * (radix - 1)
        got = call(
            functools.partial(split_kernel, rows, shift, radix, len(recvs), int(tail)),
            [acc, *recvs],
            outs,
        )
        acc = got[0]
        recvs = [swap(s, "tp", tp, k << shift) for k, s in zip(SCATTER_ORDER[radix], got[1:])]
    return acc, recvs


def paired_scatter_rounds(keep, send, rows, tp, order, tail):
    width = keep.shape[1]
    acc, recvs = keep, [swap(send, "tp", tp, 1)]
    for shift, radix in digits_of(tp, 1)[1:]:
        n = acc.shape[0]
        if radix != 4:
            acc, out = call(
                functools.partial(split_kernel, rows, shift, radix, len(recvs), int(tail)),
                [acc, *recvs],
                [sds((n // radix, width), f32), sds((n // radix, width), bf16)],
            )
            recvs = [swap(out, "tp", tp, 1 << shift)]
            continue
        acc, out = call(
            functools.partial(first_half_kernel, rows, shift, order, len(recvs), int(tail)),
            [acc, *recvs],
            [sds((n // 2, width), f32), sds((n // 2, width), bf16)],
        )
        recv = swap(out, "tp", tp, order[0] << shift)
        acc, out = call(
            functools.partial(second_half_kernel, int(tail)),
            [acc, recv],
            [sds((n // 4, width), f32), sds((n // 4, width), bf16)],
        )
        recvs = [swap(out, "tp", tp, order[1] << shift)]
    return acc, recvs


def gather_rounds(x, tp, orders):
    masks = [0]
    for shift, radix in digits_of(tp, 1)[1:]:
        order = orders[radix]
        x = jnp.concatenate([x] + [swap(x, "tp", tp, k << shift) for k in order], axis=0)
        masks = [m | (k << shift) for k in (0, *order) for m in masks]
    return x, swap(x, "tp", tp, 1), masks


def sum_terms(part, kv):
    digits = digits_of(kv)
    terms = [part]
    for i, (shift, radix) in enumerate(digits):
        if i:
            part = tree([t.astype(f32) for t in terms]).astype(bf16)
        terms = [part] + [swap(part, "kv", kv, k << shift) for k in range(1, radix)]
    return terms


def solution(mesh):
    tp, kv = mesh.shape["tp"], mesh.shape["kv"]

    def body(
        tokens,
        norm_gain,
        query_weight,
        key_weight,
        value_weight,
        input_gate_weight,
        forget_gate_weight,
        input_gate_bias,
        forget_gate_bias,
        memory_state,
        normalizer_state,
        stabilizer_state,
        block_keys,
        block_values,
        block_input_pre,
        block_forget_pre,
        block_lengths,
        head_norm_gain,
        output_weight,
        mixer_norm_gain,
        gate_weight,
        up_weight,
        down_weight,
    ):
        total, depth = tokens.shape
        seqs, heads, block, size = block_keys.shape
        width = heads * size
        model = depth * tp
        all_heads = input_gate_weight.shape[1]
        half = total // 2
        bias_i, bias_f = input_gate_bias[None, :], forget_gate_bias[None, :]

        packed = 3 * width + LANES
        keep, send = call(
            functools.partial(project_kernel, seqs),
            [
                tokens,
                norm_gain[None, :],
                query_weight,
                key_weight,
                value_weight,
                input_gate_weight.T,
                forget_gate_weight.T,
            ],
            [sds((half, packed), f32), sds((half, packed), bf16)],
            [
                sds((total, depth), bf16),
                sds((1, depth), f32),
                *[sds((depth, width), bf16)] * 3,
                *[sds((all_heads, depth), bf16)] * 2,
                sds((total, depth), bf16),
            ],
            fetched=range(7),
            copies=7,
        )
        acc, recvs = scatter_rounds(keep, send, seqs, tp)
        prepared = call(
            gating_kernel,
            [
                block_input_pre,
                block_forget_pre,
                block_lengths[None, :],
                stabilizer_state.T,
                bias_i,
                bias_f,
                normalizer_state,
                head_norm_gain[None, :],
                block_keys,
                block_values,
                memory_state,
            ],
            [
                *[sds((heads * seqs, block), f32)] * 3,
                sds(block_keys.shape, bf16),
                sds(block_values.shape, bf16),
                sds(memory_state.shape, f32),
                sds(normalizer_state.shape, f32),
                sds((1, width), f32),
                sds((8, LANES), f32),
            ],
            [
                *[sds((seqs, heads, block), f32)] * 2,
                sds((1, seqs), jnp.int32),
                sds((heads, seqs), f32),
                *[sds((1, heads), f32)] * 2,
            ],
            fetched=range(11),
            copies=11,
        )
        (head_out,) = call(
            functools.partial(cell_kernel, (float(model), all_heads), len(recvs)),
            [acc, *recvs, *prepared],
            [sds((seqs, width), bf16)],
        )
        near, far, masks = gather_rounds(head_out, tp, SMALL_ORDER)
        (part,) = call(
            functools.partial(apply_kernel, masks, seqs),
            [near, far, output_weight],
            [sds((total, depth), bf16)],
            [sds((total, width), bf16)],
        )
        terms = sum_terms(part, kv)

        hidden_dev = gate_weight.shape[1]
        first = pl.cdiv(pl.cdiv(hidden_dev, LANES), HALVES) * LANES
        pieces = [(0, min(first, hidden_dev))]
        if hidden_dev > first:
            pieces.append((first, hidden_dev - first))
        packed = [2 * pl.cdiv(w, LANES) * LANES for _, w in pieces]
        packed[0] += LANES
        res, scaled, *split = call(
            functools.partial(mixer_kernel, seqs, pieces[0][1], len(terms)),
            [*terms, tokens, mixer_norm_gain[None, :], gate_weight, up_weight],
            [
                sds((total, depth), f32),
                sds((total, depth), bf16),
                sds((half, packed[0]), f32),
                sds((half, packed[0]), bf16),
            ],
            [sds((total, depth), f32)],
        )
        scales = part = None
        for i, (at, w) in enumerate(pieces):
            if i:
                split = call(
                    functools.partial(rest_kernel, at, w),
                    [scaled, gate_weight, up_weight],
                    [sds((half, packed[i]), f32), sds((half, packed[i]), bf16)],
                )
            acc, recvs = paired_scatter_rounds(*split, seqs, tp, ((1, 3), (3, 1))[i], i == 0)
            got = call(
                functools.partial(activate_kernel, float(model), len(recvs), i == 0),
                [acc, *recvs] + ([scales] if i else []),
                [sds((seqs, w), bf16)] + ([] if i else [sds((seqs, LANES), f32)]),
            )
            if i == 0:
                scales = got[1]
            near, far, masks = gather_rounds(got[0], tp, LARGE_ORDER)
            last = i == len(pieces) - 1
            (part,) = call(
                functools.partial(down_kernel, masks, seqs, at, i > 0),
                [near, far, down_weight] + ([part] if i else []),
                [sds((total, depth), bf16 if last else f32)],
                [sds((total, w), bf16)],
            )
        terms = sum_terms(part, kv)
        return res + tree([t.astype(f32) for t in terms])

    placed = (
        P(None, "tp"),
        P("tp"),
        P("tp", "kv"),
        P("tp", "kv"),
        P("tp", "kv"),
        P("tp", None),
        P("tp", None),
        P("kv"),
        P("kv"),
        P("tp", "kv", None, None),
        P("tp", "kv", None),
        P("tp", "kv"),
        P("tp", "kv", None, None),
        P("tp", "kv", None, None),
        P("tp", "kv", None),
        P("tp", "kv", None),
        P("tp"),
        P("kv"),
        P("kv", "tp"),
        P("tp"),
        P("tp", "kv"),
        P("tp", "kv"),
        P("kv", "tp"),
    )
    return jax.shard_map(body, mesh=mesh, in_specs=placed, out_specs=P(None, "tp"), check_vma=False)
```
